32 devices in a mesh: sp: 16 (over z, y, x), tp: 2 (over core).
Axes of the slice: x: 2, y: 2, z: 4, core: 2. Of those that a mesh axis runs over, the one named last changes fastest.
Arguments:
- head_value_rows: bfloat16 [12288, 2048], P('sp', 'tp'), may hold values from -6 to 6
- entry_map_rows: bfloat16 [12288, 1024], P('sp', 'tp'), may hold values from -6 to 6
- readout_map_rows: bfloat16 [12288, 1024], P('sp', 'tp'), may hold values from -6 to 6
- output_gate_rows: bfloat16 [12288, 2048], P('sp', 'tp'), may hold values from -6 to 6
- step_before_softplus: bfloat16 [12288, 32], P('sp', 'tp'), may hold values from -8 to 8
- sudden_log_decay: float32 [12288, 32], P('sp', 'tp'), may hold values from -1 to 0
- document_index: int32 [12288], replicated, may hold values from 0 to 3, never falling along the last dimension, each value on 1 to 6144 neighbouring positions
- head_rate_logarithm: float32 [2, 32], P(None, 'tp'), may hold values from -30 to 0
- head_step_bias: float32 [2, 32], P(None, 'tp'), may hold values from -3 to 3
- value_conv_taps: bfloat16 [5, 2048], P(None, 'tp'), may hold values from -2.5 to 2.5
- entry_conv_taps: bfloat16 [5, 1024], P(None, 'tp'), may hold values from -2.5 to 2.5
- readout_conv_taps: bfloat16 [5, 1024], P(None, 'tp'), may hold values from -2.5 to 2.5
- group_norm_gain: float32 [2048], P('tp'), may hold values from 0.1 to 1.9
- mixer_output_weight: bfloat16 [2048, 2048], P('tp'), may hold values from -0.125 to 0.125
- stream: bfloat16 [12288, 2048], P('sp', 'tp'), may hold values from -200 to 200
- mixer_norm_gain: float32 [2048], P('tp'), may hold values from 0.1 to 1.9
- channel_norm_gain: float32 [2048], P('tp'), may hold values from 0.1 to 1.9
- up_projection_weight: bfloat16 [2048, 8192], P('sp', 'tp'), may hold values from -0.125 to 0.125
- down_projection_weight: bfloat16 [2048, 8192], P('sp', 'tp'), may hold values from -0.0625 to 0.0625
Outputs:
- mixed: bfloat16 [12288, 2048], P('sp', 'tp')
The draws below stay inside these ranges and needn't reach their ends.
All inputs are finite; a program needn't handle non-finite values.
Results may differ from the reference program's by a relative error of at most 0.018.
Values may be sent and summed in bfloat16 or wider, within the bound.
No kernel may reach another device: no remote copies, remote signals or barrier semaphores. Data moves between devices by JAX's collectives and lax.ppermute only.
A program may use at most 128 MiB of HBM per device.

```python
import math
import jax
import jax.numpy as jnp
import numpy as np
from jax import lax

D = 2048
HEADS = 32
HEAD_DIM = 64
GROUPS = 8
STATE = 128
FF = 8192
CONV_WIDTH = 5
BLOCK = 128
TOK_DEV = 768
INNER = 2048
TOKENS = 12288
N_SP = 16
N_TP = 2


def draw_step_before_softplus(key, part):
    jitter_key, shift_key = jax.random.split(key)
    jitter = jnp.clip(jax.random.normal(jitter_key, (TOKENS, HEADS), jnp.float32), -4.0, 4.0)
    shifts = jax.random.uniform(shift_key, (TOKENS // TOK_DEV, 1, HEADS), jnp.float32, -1.0, 1.5)
    shifts = jnp.broadcast_to(shifts, (TOKENS // TOK_DEV, TOK_DEV, HEADS)).reshape(TOKENS, HEADS)
    return (jitter + shifts).astype(jnp.bfloat16)


def draw_head_rate_logarithm(key, part):
    pick_key, slow_key, fast_key = jax.random.split(key, 3)
    quick = jax.random.randint(pick_key, (2, HEADS), 0, 2) == 1
    slow_rate = jax.random.uniform(slow_key, (2, HEADS), jnp.float32, math.log(0.1), math.log(0.5))
    slow_rate = slow_rate - jnp.log(jnp.float32(TOKENS))
    fast_rate = jax.random.uniform(fast_key, (2, HEADS), jnp.float32, math.log(0.01), math.log(1.0 / 30.0))
    return jnp.where(quick, fast_rate, slow_rate)


def draw_sudden_log_decay(key, part):
    where_key, depth_key = jax.random.split(key)
    struck = jax.random.randint(where_key, (TOKENS, 1), 0, TOKENS) < 4
    depth = jax.random.uniform(depth_key, (TOKENS, HEADS), jnp.float32, math.log(0.5), math.log(0.8))
    return jnp.where(struck, depth, 0.0)


def draw_stream(key, part):
    base_key, row_key = jax.random.split(key, 2)
    col_scale = 3.0 ** (jnp.arange(D, dtype=jnp.float32) / D - 0.5)
    values = jnp.clip(jax.random.normal(base_key, (TOKENS, D), jnp.float32), -6.0, 6.0)
    row_scale = jnp.exp(jax.random.uniform(row_key, (TOKENS, 1), jnp.float32, math.log(0.5), math.log(2.0)))
    return (values * row_scale * col_scale).astype(jnp.bfloat16)


def levels(stream_key, shape, cuts, low, largest):
    loudness = 1.0
    for axis_at, blocks in cuts:
        heights = jax.random.uniform(jax.random.fold_in(jax.random.fold_in(stream_key, 6), axis_at), (blocks,), jnp.float32, low / len(cuts), largest / len(cuts))
        loudness = loudness * jnp.repeat(jnp.exp(heights), shape[axis_at] // blocks).reshape((-1,) + (1,) * (len(shape) - 1 - axis_at))
    return loudness


def split_up(amount, total, bound, skew):
    weights = [(1 << 20) // math.isqrt(grade ** skew) + 1 for grade in range(2, amount + 1)]
    spare, holding = total - bound - (amount - 1), [1] * (amount - 1)
    while spare > 0:
        movable = [i for i in range(amount - 1) if holding[i] < bound]
        pool, remaining = sum([weights[i] for i in movable]), spare
        for i in movable:
            more = min(bound - holding[i], max(1, remaining * weights[i] // pool), spare)
            holding[i] = holding[i] + more
            spare = spare - more
    return np.array([bound] + holding)


def ragged_sizes(key, amount, total, reach, skew):
    if amount == 2:
        one = jax.random.randint(key, (), max(1, total - reach), min(reach, total - 1) + 1)
        return jnp.stack([one, total - one])
    sizes = jnp.asarray(split_up(amount, total, reach, skew), jnp.int32)
    twos = (amount - 1) // 2
    donor, receiver = sizes[1:1 + 2 * twos:2], sizes[2:2 + 2 * twos:2]
    margin = jnp.minimum(donor - 1, reach - receiver)
    shifted = jax.random.randint(jax.random.fold_in(key, 1), (twos,), 0, 1 << 20) % (margin + 1)
    sizes = sizes.at[1:1 + 2 * twos:2].set(donor - shifted).at[2:2 + 2 * twos:2].set(receiver + shifted)
    return sizes[jax.random.permutation(jax.random.fold_in(key, 2), amount)]


def noise(own_key, extent, deviation, most, cuts=(), kind=jnp.bfloat16):
    loudness = levels(own_key, extent, cuts, -0.22, 0.18) if cuts else 1.0
    values = jax.random.normal(own_key, extent, jnp.float32) * deviation * loudness
    return jnp.minimum(jnp.maximum(values, -most), most).astype(kind)


def setup_inputs(seed: int = 0) -> dict:
    arg_keys = jax.random.split(jax.random.key(seed), 20)
    return {
        "head_value_rows": noise(arg_keys[0], (TOKENS, INNER), 1.0, 6.0, ((0, 16), (1, 2))),
        "entry_map_rows": noise(arg_keys[1], (TOKENS, GROUPS * STATE), 1.0, 6.0, ((0, 16), (1, 2))),
        "readout_map_rows": noise(arg_keys[2], (TOKENS, GROUPS * STATE), 1.0, 6.0, ((0, 16), (1, 2))),
        "output_gate_rows": noise(arg_keys[3], (TOKENS, INNER), 1.0, 6.0, ((0, 16), (1, 2))),
        "step_before_softplus": draw_step_before_softplus(jax.random.fold_in(arg_keys[19], 71), 0),
        "sudden_log_decay": draw_sudden_log_decay(jax.random.fold_in(arg_keys[19], 71), 0),
        "document_index": jnp.searchsorted(jnp.cumsum(ragged_sizes(arg_keys[6], N_SP // 4, TOKENS, 8 * TOK_DEV, 1)), jnp.arange(TOKENS), side="right").astype(jnp.int32),
        "head_rate_logarithm": draw_head_rate_logarithm(jax.random.fold_in(arg_keys[19], 71), 0),
        "head_step_bias": noise(arg_keys[8], (2, HEADS), 0.5, 3.0, ((1, 2),), jnp.float32),
        "value_conv_taps": noise(arg_keys[9], (CONV_WIDTH, INNER), CONV_WIDTH ** -0.5, 2.5, ((1, 2),)),
        "entry_conv_taps": noise(arg_keys[10], (CONV_WIDTH, GROUPS * STATE), CONV_WIDTH ** -0.5, 2.5, ((1, 2),)),
        "readout_conv_taps": noise(arg_keys[11], (CONV_WIDTH, GROUPS * STATE), CONV_WIDTH ** -0.5, 2.5, ((1, 2),)),
        "group_norm_gain": jnp.clip(1.0 + 0.18 * jax.random.normal(arg_keys[12], (INNER,), jnp.float32), 0.1, 1.9),
        "mixer_output_weight": noise(arg_keys[13], (INNER, D), INNER ** -0.5, 0.125, ((0, 2),)),
        "stream": draw_stream(jax.random.fold_in(arg_keys[19], 71), 0),
        "mixer_norm_gain": jnp.clip(1.0 + 0.18 * jax.random.normal(arg_keys[15], (D,), jnp.float32), 0.1, 1.9),
        "channel_norm_gain": jnp.clip(1.0 + 0.18 * jax.random.normal(arg_keys[16], (D,), jnp.float32), 0.1, 1.9),
        "up_projection_weight": noise(arg_keys[17], (D, FF), D ** -0.5, 0.125, ((0, 16), (1, 2))),
        "down_projection_weight": noise(arg_keys[18], (D, FF), FF ** -0.5, 0.0625, ((0, 16), (1, 2))),
    }


exact_prec = lax.Precision.HIGHEST
norm_eps = 1e-05
resid_scale = 1.4142135623730951

def block_step(running, blocks):
    states, last_doc = running
    scaled, entries, readout, decay_logarithm, block_ids = blocks
    block_len = block_ids.shape[0]
    cum_decay = jnp.cumsum(decay_logarithm, axis=0)
    indices = lax.iota(jnp.int32, block_len)
    linked = (indices[:, None] >= indices[None, :]) & (block_ids[:, None] == block_ids[None, :])
    link_mask = linked[:, :, None, None]
    spread = cum_decay[:, None] - cum_decay[None, :]
    weights = jnp.where(link_mask, jnp.exp(jnp.where(link_mask, spread, 0.0)), 0.0)
    scores = jnp.einsum('tgn,sgn->tsg', readout, entries, precision=exact_prec)
    within = jnp.einsum('tsg,tsgr,sgrp->tgrp', scores, weights, scaled, precision=exact_prec)
    arrival = jnp.where((block_ids == last_doc)[:, None, None], jnp.exp(cum_decay), 0.0)
    carried = jnp.einsum('tgn,grpn->tgrp', readout, states, precision=exact_prec) * arrival[..., None]
    end_doc = block_ids[-1]
    to_end = jnp.where((block_ids == end_doc)[:, None, None], jnp.exp(cum_decay[-1] - cum_decay), 0.0)
    passing = jnp.where(end_doc == last_doc, jnp.exp(cum_decay[-1]), 0.0)
    fresh = jnp.einsum('sgn,sgr,sgrp->grpn', entries, to_end, scaled, precision=exact_prec)
    return ((states * passing[..., None, None] + fresh, end_doc), within + carried)

def sweep_blocks(scaled, entries, readout, decay_logarithm, document_index, states, last_doc, block_len):
    row_count = document_index.shape[0]
    block_count = row_count // block_len

    def in_blocks(array):
        return array.reshape((block_count, block_len) + array.shape[1:])
    inputs = tuple((in_blocks(array) for array in (scaled, entries, readout, decay_logarithm, document_index)))
    (states, last_doc), output = lax.scan(block_step, (states, last_doc), inputs)
    return (output.reshape((row_count,) + output.shape[2:]), states)

def short_conv(inputs, weights, document_index):
    taps = weights.shape[0]
    half_width = taps // 2
    row_count = inputs.shape[0]
    padded = jnp.pad(inputs, ((half_width, half_width), (0, 0)))
    doc_pad = jnp.pad(document_index, half_width, constant_values=-1)
    summed = jnp.zeros(inputs.shape, jnp.float32)
    for offset in range(taps):
        same_doc = (doc_pad[offset:offset + row_count] == document_index)[:, None]
        summed = summed + weights[offset] * jnp.where(same_doc, padded[offset:offset + row_count], 0.0)
    return jax.nn.silu(summed)

def layer_norm(residual, gain):
    row_mean = lax.optimization_barrier(jnp.mean(residual, axis=1))
    row_var = lax.optimization_barrier(jnp.mean(residual * residual, axis=1)) - row_mean * row_mean
    return ((residual - row_mean[:, None]) * lax.rsqrt(row_var + norm_eps)[:, None] * gain).astype(jnp.bfloat16)

def block_sums(left, right):
    parts = jnp.einsum('tjc,jcd->jtd', left, right)
    rounded = parts.astype(jnp.bfloat16)
    rounded = lax.optimization_barrier(rounded)
    return lax.optimization_barrier(jnp.sum(rounded.astype(jnp.float32), axis=0))

def reference(head_value_rows, entry_map_rows, readout_map_rows, output_gate_rows, step_before_softplus, sudden_log_decay, document_index, head_rate_logarithm, head_step_bias, value_conv_taps, entry_conv_taps, readout_conv_taps, group_norm_gain, mixer_output_weight, stream, mixer_norm_gain, channel_norm_gain, up_projection_weight, down_projection_weight):
    per_group = HEADS // GROUPS
    values = short_conv(head_value_rows.astype(jnp.float32), value_conv_taps.astype(jnp.float32), document_index)
    values = values.reshape(TOKENS, GROUPS, per_group, HEAD_DIM)
    entries = short_conv(entry_map_rows.astype(jnp.float32), entry_conv_taps.astype(jnp.float32), document_index)
    entries = entries.reshape(TOKENS, GROUPS, STATE)
    readout = short_conv(readout_map_rows.astype(jnp.float32), readout_conv_taps.astype(jnp.float32), document_index)
    readout = readout.reshape(TOKENS, GROUPS, STATE)
    summed = jnp.zeros((TOKENS, GROUPS, per_group, HEAD_DIM), jnp.float32)
    for sweep_direction in range(2):
        head_step_length = jax.nn.softplus(step_before_softplus.astype(jnp.float32) + head_step_bias[sweep_direction])
        decay_logarithm = -jnp.exp(head_rate_logarithm[sweep_direction]) * head_step_length + sudden_log_decay
        decay_logarithm = decay_logarithm.reshape(TOKENS, GROUPS, per_group)
        scaled = values * head_step_length.reshape(TOKENS, GROUPS, per_group)[..., None]
        arrays = (scaled, entries, readout, decay_logarithm, document_index)
        if sweep_direction == 1:
            arrays = tuple((jnp.flip(array, 0) for array in arrays))
        start_state = jnp.zeros((GROUPS, per_group, HEAD_DIM, STATE), jnp.float32)
        output, _ = sweep_blocks(*arrays, start_state, jnp.int32(-1), BLOCK)
        if sweep_direction == 1:
            output = jnp.flip(output, 0)
        summed = summed + output
    gated = summed.reshape(TOKENS, GROUPS, per_group * HEAD_DIM)
    gated = gated * jax.nn.silu(output_gate_rows.astype(jnp.float32)).reshape(TOKENS, GROUPS, per_group * HEAD_DIM)
    gated = gated * lax.rsqrt(lax.optimization_barrier(jnp.mean(gated * gated, axis=2, keepdims=True)) + norm_eps)
    normed = (gated.reshape(TOKENS, INNER) * group_norm_gain).astype(jnp.bfloat16)
    out_blocks = mixer_output_weight.astype(jnp.float32).reshape(N_TP, INNER // N_TP, D)
    down_blocks = down_projection_weight.astype(jnp.float32).reshape(D, N_TP, FF // N_TP)

    def dense_rows(pieces):
        normed_rows, stream_rows = pieces
        mixer_sum = block_sums(normed_rows.astype(jnp.float32).reshape(-1, N_TP, INNER // N_TP), out_blocks)
        first_sum = resid_scale * stream_rows.astype(jnp.float32) + mixer_sum
        normed_one = layer_norm(first_sum, mixer_norm_gain)
        hidden = jnp.dot(normed_one, up_projection_weight, preferred_element_type=jnp.float32)
        squared = jnp.square(jax.nn.relu(hidden)).astype(jnp.bfloat16)
        parts = jnp.einsum('tjf,djf->jtd', squared.astype(jnp.float32).reshape(-1, N_TP, FF // N_TP), down_blocks)
        rounded = lax.optimization_barrier(parts.astype(jnp.bfloat16))
        down_sum = lax.optimization_barrier(jnp.sum(rounded.astype(jnp.float32), axis=0))
        second_sum = resid_scale * normed_one.astype(jnp.float32) + down_sum
        return layer_norm(second_sum, channel_norm_gain)
    result = lax.map(dense_rows, (normed.reshape(N_SP, TOK_DEV, INNER), stream.reshape(N_SP, TOK_DEV, D)))
    return result.reshape(TOKENS, D)
```

```python
import jax
import jax.numpy as jnp
from jax import lax
from jax.experimental import pallas as pl
from jax.experimental.pallas import tpu as pltpu
from jax.sharding import PartitionSpec as P

HEAD_DIM = 64
STATE = 128
BLOCK = 128
MAX_DOCUMENT = 6144
LOG2E = 1.4426950408889634

exact_prec = lax.Precision.HIGHEST
norm_eps = 1e-05
resid_scale = 1.4142135623730951
f32 = jnp.float32
bf16 = jnp.bfloat16


def shifted(array, axis, by):
    count = lax.axis_size(axis)
    pairs = [(i, i + by) for i in range(count) if 0 <= i + by < count]
    return lax.ppermute(array, axis, pairs)


def over_tp(array):
    count = lax.axis_size("tp")
    if count == 1:
        return [array]
    return [array, lax.ppermute(array, "tp", [(0, 1), (1, 0)])]


def columns_over_tp(array):
    count = lax.axis_size("tp")
    if count == 1:
        return array
    own, other = over_tp(array)
    first = lax.axis_index("tp") == 0
    return jnp.concatenate(
        [jnp.where(first, own, other), jnp.where(first, other, own)], axis=1
    )


def norm_scattered(part, residual, gain):
    added = lax.psum_scatter(part, "tp", scatter_dimension=1, tiled=True).astype(f32)
    total = resid_scale * residual.astype(f32) + added
    width = part.shape[1]
    sums = lax.psum((jnp.sum(total, axis=1), jnp.sum(total * total, axis=1)), "tp")
    mean = sums[0] / width
    variance = sums[1] / width - mean * mean
    return ((total - mean[:, None]) * lax.rsqrt(variance + norm_eps)[:, None] * gain).astype(bf16)


def spread(columns, heads_per):
    rows = columns.shape[0]
    lane = lax.broadcasted_iota(jnp.int32, (rows, 2 * HEAD_DIM), 1)
    pieces = []
    for pair in range(heads_per // 2):
        low = columns[:, 2 * pair : 2 * pair + 1]
        high = columns[:, 2 * pair + 1 : 2 * pair + 2]
        pieces.append(jnp.where(lane < HEAD_DIM, low, high))
    return jnp.concatenate(pieces, axis=1)


def mixer_kernel(
    value_ref, entry_ref, readout_ref,
    low_value_ref, low_entry_ref, low_readout_ref,
    high_value_ref, high_entry_ref, high_readout_ref,
    value_tap_ref, entry_tap_ref, readout_tap_ref,
    mask_ref, doc_row_ref, column_ref, row_ref, pass_ref,
    out_ref, readout_out_ref, end_ref,
    window, values, entries, fresh, starts,
):
    rows, width = value_ref.shape
    per = width // HEAD_DIM
    blocks = rows // BLOCK
    taps = value_tap_ref.shape[0]
    half = taps // 2
    edge = 8
    pieces = [(value_ref, low_value_ref, high_value_ref, value_tap_ref, i * 128, i * 128)
              for i in range(width // 128)]
    pieces.append((entry_ref, low_entry_ref, high_entry_ref, entry_tap_ref, 0, width))
    pieces.append((readout_ref, low_readout_ref, high_readout_ref, readout_tap_ref, 0, width + 128))
    for source, low, high, _, at, to in pieces:
        window[0:edge, to : to + 128] = low[:, at : at + 128].astype(f32)
        window[edge + rows : 2 * edge + rows, to : to + 128] = high[:, at : at + 128].astype(f32)
        window[edge : edge + rows, to : to + 128] = source[:, at : at + 128].astype(f32)

    def conv_block(b, _):
        start = pl.multiple_of(b * BLOCK, BLOCK)
        here = pl.ds(start, BLOCK)
        masks = mask_ref[here, :]
        columns = column_ref[here, :]
        value_parts = []
        for source, low, high, tap_ref, at, to in pieces:
            around = window[pl.ds(start, BLOCK + 2 * edge), to : to + 128]
            total = jnp.zeros((BLOCK, 128), f32)
            for k in range(taps):
                moved = around[edge - half + k : edge - half + k + BLOCK]
                term = moved * tap_ref[k : k + 1, at : at + 128].astype(f32)
                if k != half:
                    term = term * masks[:, k : k + 1]
                total = total + term
            active = 0.5 * total * (1.0 + jnp.tanh(0.5 * total))
            if to < width:
                value_parts.append(active)
            elif to == width:
                entry = active.astype(bf16)
            else:
                readout_out_ref[here, :] = active.astype(bf16)
        value = jnp.concatenate(value_parts, axis=1)
        values[here, :] = value.astype(bf16)
        entries[here, :] = entry
        forward = value * spread(columns[:, 2 * per : 3 * per], per)
        backward = value * spread(columns[:, 3 * per : 4 * per], per)
        weighted = jnp.concatenate([forward, backward], axis=1).astype(bf16)
        fresh[b] = lax.dot_general(
            entry, weighted, (((0,), (0,)), ((), ())), preferred_element_type=f32
        )
        return 0

    lax.fori_loop(0, blocks, conv_block, 0)

    state = jnp.zeros((STATE, width), f32)
    for b in range(blocks):
        starts[b, :, 0:width] = state.astype(bf16)
        state = state * pass_ref[b, 0:1, :] + fresh[b, :, 0:width]
    end_ref[0] = state.astype(bf16)
    state = jnp.zeros((STATE, width), f32)
    for b in range(blocks - 1, -1, -1):
        starts[b, :, width : 2 * width] = state.astype(bf16)
        state = state * pass_ref[b, 1:2, :] + fresh[b, :, width : 2 * width]
    end_ref[1] = state.astype(bf16)

    def out_block(b, _):
        start = pl.multiple_of(b * BLOCK, BLOCK)
        here = pl.ds(start, BLOCK)
        columns = column_ref[here, :]
        along = row_ref[b]
        readout = readout_out_ref[here, :]
        entry = entries[here, :]
        value = values[here, :]
        at = lax.broadcasted_iota(jnp.int32, (BLOCK, BLOCK), 0)
        source = lax.broadcasted_iota(jnp.int32, (BLOCK, BLOCK), 1)
        scores = lax.dot_general(
            readout, entry, (((1,), (1,)), ((), ())), preferred_element_type=f32
        )
        same = mask_ref[here, 5:6] == doc_row_ref[b]
        scores = jnp.where(same, scores, 0.0)
        lane = lax.broadcasted_iota(jnp.int32, (BLOCK, width), 1)
        weights = []
        spreads = []
        for r in range(per):
            ahead = columns[:, r : r + 1] + along[r : r + 1, :]
            behind = columns[:, per + r : per + r + 1] + along[per + r : per + r + 1, :]
            both = along[2 * per + r : 2 * per + r + 1, :]
            power = jnp.where(at > source, ahead, jnp.where(at < source, behind, both))
            weights.append((scores * jnp.exp2(power)).astype(bf16))
            own = (lane >= r * HEAD_DIM) & (lane < (r + 1) * HEAD_DIM)
            spreads.append(jnp.where(own, value, jnp.zeros_like(value)))
        total = jnp.dot(
            jnp.concatenate(weights, axis=1),
            jnp.concatenate(spreads, axis=0),
            preferred_element_type=f32,
        )
        carried = jnp.dot(readout, starts[b], preferred_element_type=f32)
        total = total + carried[:, 0:width] * spread(columns[:, 4 * per : 5 * per], per)
        total = total + carried[:, width : 2 * width] * spread(columns[:, 5 * per : 6 * per], per)
        out_ref[here, :] = total
        return 0

    lax.fori_loop(0, blocks, out_block, 0)


def gate_kernel(mixed_ref, readout_ref, state_ref, column_ref, gate_ref, gain_ref, out_ref):
    rows, width = mixed_ref.shape
    per = width // HEAD_DIM

    def one(b, _):
        here = pl.ds(pl.multiple_of(b * BLOCK, BLOCK), BLOCK)
        columns = column_ref[here, :]
        carried = jnp.dot(readout_ref[here, :], state_ref[...], preferred_element_type=f32)
        total = mixed_ref[here, :]
        total = total + carried[:, 0:width] * spread(columns[:, 6 * per : 7 * per], per)
        total = total + carried[:, width : 2 * width] * spread(columns[:, 7 * per : 8 * per], per)
        gate = gate_ref[here, :].astype(f32)
        total = total * (0.5 * gate * (1.0 + jnp.tanh(0.5 * gate)))
        scale = lax.rsqrt(jnp.mean(total * total, axis=1, keepdims=True) + norm_eps)
        out_ref[here, :] = (total * scale * gain_ref[...]).astype(bf16)
        return 0

    lax.fori_loop(0, rows // BLOCK, one, 0)


def norm_kernel(*refs):
    parts, (stream_ref, gain_ref, out_ref) = refs[:-3], refs[-3:]
    total = resid_scale * stream_ref[...].astype(f32)
    added = parts[0][...].astype(f32)
    for part in parts[1:]:
        added = added + part[...].astype(f32)
    total = total + added
    width = total.shape[1]
    mean = jnp.sum(total, axis=1, keepdims=True) / width
    variance = jnp.sum(total * total, axis=1, keepdims=True) / width - mean * mean
    out_ref[...] = ((total - mean) * lax.rsqrt(variance + norm_eps) * gain_ref[...]).astype(bf16)


def norm_rows(parts, stream, gain):
    rows, width = stream.shape
    tile = min(rows, BLOCK)
    spec = pl.BlockSpec((tile, width), lambda i: (i, 0))
    return pl.pallas_call(
        norm_kernel,
        grid=(rows // tile,),
        in_specs=[spec] * (len(parts) + 1) + [pl.BlockSpec((1, width), lambda i: (0, 0))],
        out_specs=spec,
        out_shape=jax.ShapeDtypeStruct((rows, width), bf16),
        name="norm_rows",
    )(*parts, stream, gain)


def by_group(array, groups):
    return array.reshape(array.shape[0], groups, -1).transpose(1, 0, 2)


def per_device(
    head_value_rows,
    entry_map_rows,
    readout_map_rows,
    output_gate_rows,
    step_before_softplus,
    sudden_log_decay,
    document_index,
    head_rate_logarithm,
    head_step_bias,
    value_conv_taps,
    entry_conv_taps,
    readout_conv_taps,
    group_norm_gain,
    mixer_output_weight,
    stream,
    mixer_norm_gain,
    channel_norm_gain,
    up_projection_weight,
    down_projection_weight,
):
    up_full = lax.all_gather(up_projection_weight, "sp", axis=0, tiled=True)
    down_full = lax.all_gather(down_projection_weight, "sp", axis=0, tiled=True)
    row_count = head_value_rows.shape[0]
    head_count = step_before_softplus.shape[1]
    groups = entry_map_rows.shape[1] // STATE
    per = head_count // groups
    width = per * HEAD_DIM
    blocks = row_count // BLOCK
    taps = value_conv_taps.shape[0]
    half = taps // 2
    edge = 8

    joined_low = jnp.concatenate(
        [a[-edge:] for a in (head_value_rows, entry_map_rows, readout_map_rows)], axis=1
    )
    joined_high = jnp.concatenate(
        [a[:edge] for a in (head_value_rows, entry_map_rows, readout_map_rows)], axis=1
    )
    low = shifted(joined_low, "sp", 1)
    high = shifted(joined_high, "sp", -1)
    splits = (head_value_rows.shape[1], head_value_rows.shape[1] + entry_map_rows.shape[1])
    low_parts = jnp.split(low, splits, axis=1)
    high_parts = jnp.split(high, splits, axis=1)

    position = lax.axis_index("sp") * row_count
    doc_pad = jnp.pad(document_index, half, constant_values=-1)
    window_ids = lax.dynamic_slice_in_dim(doc_pad, position, row_count + 2 * half)
    own_ids = window_ids[half : half + row_count]
    prev_id = window_ids[half - 1]
    next_id = window_ids[half + row_count]
    block_ids = own_ids.reshape(blocks, BLOCK)
    first_ids, last_ids = block_ids[:, 0], block_ids[:, -1]
    none = jnp.full((1,), -1, jnp.int32)
    before_ids = jnp.concatenate([none, last_ids[:-1]])
    after_ids = jnp.concatenate([first_ids[1:], none])
    mask_columns = [(window_ids[k : k + row_count] == own_ids).astype(f32) for k in range(taps)]
    masks = jnp.stack(mask_columns + [own_ids.astype(f32)] * (8 - taps), axis=1)
    doc_rows = block_ids.astype(f32)[:, None, :]

    raw = step_before_softplus.astype(f32)
    steps = [jax.nn.softplus(raw + head_step_bias[k]) for k in range(2)]
    decays = [
        (-jnp.exp(head_rate_logarithm[k]) * steps[k] + sudden_log_decay).reshape(
            blocks, BLOCK, head_count
        ) * LOG2E
        for k in range(2)
    ]
    at = lax.iota(jnp.int32, BLOCK)
    lower = (at[:, None] >= at[None, :]).astype(f32)
    cum_fwd = jnp.einsum("ts,bsh->bth", lower, decays[0], precision=exact_prec)
    cum_bwd = jnp.einsum("st,bsh->bth", lower, decays[1], precision=exact_prec)
    block_steps = [s.reshape(blocks, BLOCK, head_count) for s in steps]
    total_fwd = cum_fwd[:, -1]
    total_bwd = cum_bwd[:, 0]
    before_fwd = jnp.cumsum(total_fwd, axis=0) - total_fwd
    after_bwd = jnp.cumsum(total_bwd[::-1], axis=0)[::-1] - total_bwd

    def masked(condition, value):
        return jnp.where(condition[..., None], value, 0.0)

    to_end = masked(block_ids == last_ids[:, None], jnp.exp2(total_fwd[:, None] - cum_fwd) * block_steps[0])
    to_start = masked(block_ids == first_ids[:, None], jnp.exp2(total_bwd[:, None] - cum_bwd) * block_steps[1])
    arrive_fwd = masked(block_ids == before_ids[:, None], jnp.exp2(cum_fwd))
    arrive_bwd = masked(block_ids == after_ids[:, None], jnp.exp2(cum_bwd))
    far_fwd = masked(block_ids == prev_id, jnp.exp2(cum_fwd + before_fwd[:, None]))
    far_bwd = masked(block_ids == next_id, jnp.exp2(cum_bwd + after_bwd[:, None]))
    columns = jnp.stack(
        [cum_fwd, cum_bwd, to_end, to_start, arrive_fwd, arrive_bwd, far_fwd, far_bwd]
    ).reshape(8, row_count, groups, per).transpose(2, 1, 0, 3).reshape(groups, row_count, 8 * per)
    along = jnp.stack(
        [
            jnp.log2(block_steps[0]) - cum_fwd,
            jnp.log2(block_steps[1]) - cum_bwd,
            jnp.log2(block_steps[0] + block_steps[1]),
            jnp.zeros_like(cum_fwd),
        ]
    ).reshape(4, blocks, BLOCK, groups, per).transpose(3, 1, 0, 4, 2).reshape(groups, blocks, 4 * per, BLOCK)
    pass_fwd = masked(last_ids == before_ids, jnp.exp2(total_fwd))
    pass_bwd = masked(first_ids == after_ids, jnp.exp2(total_bwd))
    passes = jnp.stack([pass_fwd, pass_bwd], axis=1).reshape(blocks, 2, groups, per)
    passes = jnp.repeat(passes.transpose(2, 0, 1, 3), HEAD_DIM, axis=3)

    def rows_spec(columns_wide):
        return pl.BlockSpec((row_count, columns_wide), lambda g: (0, g))

    def thin_spec(height, columns_wide):
        return pl.BlockSpec((height, columns_wide), lambda g: (0, g))

    def group_spec(*shape):
        return pl.BlockSpec((pl.Squeezed(),) + shape, lambda g: (g,) + (0,) * len(shape))

    def same_spec(*shape):
        return pl.BlockSpec(shape, lambda g: (0,) * len(shape))

    local, readouts, ends = pl.pallas_call(
        mixer_kernel,
        grid=(groups,),
        in_specs=[
            rows_spec(width), rows_spec(STATE), rows_spec(STATE),
            thin_spec(edge, width), thin_spec(edge, STATE), thin_spec(edge, STATE),
            thin_spec(edge, width), thin_spec(edge, STATE), thin_spec(edge, STATE),
            thin_spec(taps, width), thin_spec(taps, STATE), thin_spec(taps, STATE),
            same_spec(row_count, 8), same_spec(blocks, 1, BLOCK),
            group_spec(row_count, 8 * per), group_spec(blocks, 4 * per, BLOCK),
            group_spec(blocks, 2, width),
        ],
        out_specs=[
            rows_spec(width), rows_spec(STATE),
            pl.BlockSpec((2, pl.Squeezed(), STATE, width), lambda g: (0, g, 0, 0)),
        ],
        out_shape=[
            jax.ShapeDtypeStruct((row_count, groups * width), f32),
            jax.ShapeDtypeStruct((row_count, groups * STATE), bf16),
            jax.ShapeDtypeStruct((2, groups, STATE, width), bf16),
        ],
        scratch_shapes=[
            pltpu.VMEM((row_count + 2 * edge, width + 2 * STATE), f32),
            pltpu.VMEM((row_count, width), bf16),
            pltpu.VMEM((row_count, STATE), bf16),
            pltpu.VMEM((blocks, STATE, 2 * width), f32),
            pltpu.VMEM((blocks, STATE, 2 * width), bf16),
        ],
        name="mixer",
    )(
        head_value_rows, entry_map_rows, readout_map_rows, *low_parts, *high_parts,
        value_conv_taps, entry_conv_taps, readout_conv_taps,
        masks, doc_rows, columns, along, passes,
    )

    whole_fwd = jnp.where(prev_id == own_ids[-1], jnp.exp2(jnp.sum(total_fwd, axis=0)), 0.0)
    whole_bwd = jnp.where(next_id == own_ids[0], jnp.exp2(jnp.sum(total_bwd, axis=0)), 0.0)
    wide_fwd = jnp.repeat(whole_fwd.reshape(groups, 1, per), HEAD_DIM, axis=2)
    wide_bwd = jnp.repeat(whole_bwd.reshape(groups, 1, per), HEAD_DIM, axis=2)
    reach = min(lax.axis_size("sp") - 1, -(-(MAX_DOCUMENT - 1) // row_count))

    def pack(state, factor):
        coarse = factor.astype(bf16)
        fine = (factor - coarse.astype(f32)).astype(bf16)
        tail = jnp.zeros((groups, 14, width), bf16)
        return jnp.concatenate([state.astype(bf16), coarse, fine, tail], axis=1)

    def unpack(packed):
        factor = packed[:, STATE : STATE + 1].astype(f32)
        factor = factor + packed[:, STATE + 1 : STATE + 2].astype(f32)
        return packed[:, :STATE].astype(f32), factor

    def chain(earlier, later):
        return earlier[0] * later[1] + later[0], earlier[1] * later[1]

    firsts = []
    for state, factor, sign in ((ends[0], wide_fwd, 1), (ends[1], wide_bwd, -1)):
        packed = pack(state, factor)
        firsts.append((sign, shifted(packed, "sp", sign), shifted(packed, "sp", 2 * sign)))
    seconds = []
    for sign, near, far in firsts:
        gathered = chain(unpack(far), unpack(near))
        packed = pack(*gathered)
        seconds.append((gathered, [shifted(packed, "sp", sign * j) for j in range(2, reach, 2)]))
    arrived = []
    for gathered, more in seconds:
        total = gathered
        for other in more:
            total = chain(unpack(other), total)
        arrived.append(total[0].astype(bf16))
    incoming = jnp.concatenate(arrived, axis=2)

    normed = pl.pallas_call(
        gate_kernel,
        grid=(groups,),
        in_specs=[
            rows_spec(width), rows_spec(STATE), group_spec(STATE, 2 * width),
            group_spec(row_count, 8 * per), rows_spec(width), thin_spec(1, width),
        ],
        out_specs=rows_spec(width),
        out_shape=jax.ShapeDtypeStruct((row_count, groups * width), bf16),
        name="gate",
    )(local, readouts, incoming, columns, output_gate_rows, group_norm_gain[None])

    part = jnp.dot(normed, mixer_output_weight, preferred_element_type=f32).astype(bf16)
    own_width = stream.shape[1]
    if lax.axis_size("tp") <= 2:
        stream_full = columns_over_tp(stream)
        gain_one = columns_over_tp(mixer_norm_gain[None])
        normed_one = norm_rows(over_tp(part), stream_full, gain_one)
    else:
        own_one = norm_scattered(part, stream, mixer_norm_gain)
        normed_one = lax.all_gather(own_one, "tp", axis=1, tiled=True)
    hidden = jnp.dot(normed_one, up_full, preferred_element_type=f32)
    squared = jnp.square(jax.nn.relu(hidden)).astype(bf16)
    down_part = lax.dot_general(
        squared, down_full, (((1,), (1,)), ((), ())), preferred_element_type=f32
    ).astype(bf16)
    if lax.axis_size("tp") > 2:
        return norm_scattered(down_part, own_one, channel_norm_gain)
    gain_two = columns_over_tp(channel_norm_gain[None])
    mixed = norm_rows(over_tp(down_part), normed_one, gain_two)
    return lax.dynamic_slice_in_dim(mixed, lax.axis_index("tp") * own_width, own_width, axis=1)


def solution(mesh):
    both = P("sp", "tp")
    second = P(None, "tp")
    placed = (
        both, both, both, both, both, both, P(), second, second, second, second, second,
        P("tp"), P("tp", None), both, P("tp"), P("tp"), both, both,
    )
    return jax.shard_map(
        per_device, mesh=mesh, in_specs=placed, out_specs=both, check_vma=False
    )
```

```python
import jax
import jax.numpy as jnp
from jax import lax
from jax.experimental import pallas as pl
from jax.experimental.pallas import tpu as pltpu
from jax.sharding import PartitionSpec as P

HEAD_DIM = 64
STATE = 128
BLOCK = 128
MAX_DOCUMENT = 6144
LOG2E = 1.4426950408889634

exact_prec = lax.Precision.HIGHEST
norm_eps = 1e-05
resid_scale = 1.4142135623730951
f32 = jnp.float32
bf16 = jnp.bfloat16


SP = ("outer", "inner")


def shifted(array, by):
    count = lax.axis_size(SP)
    pairs = [(i, i + by) for i in range(count) if 0 <= i + by < count]
    return lax.ppermute(array, SP, pairs)


def partner(array, turn):
    return lax.ppermute(array, "inner", [(i, i ^ turn) for i in range(lax.axis_size("inner"))])


def over_tp(array):
    count = lax.axis_size("tp")
    if count == 1:
        return [array]
    return [array, lax.ppermute(array, "tp", [(0, 1), (1, 0)])]


def columns_over_tp(array):
    count = lax.axis_size("tp")
    if count == 1:
        return array
    if count > 2:
        return lax.all_gather(array, "tp", axis=1, tiled=True)
    own, other = over_tp(array)
    width = array.shape[1]
    place = lax.axis_index("tp")
    joined = jnp.zeros((array.shape[0], 2 * width), array.dtype)
    joined = lax.dynamic_update_slice_in_dim(joined, own, place * width, axis=1)
    return lax.dynamic_update_slice_in_dim(joined, other, (1 - place) * width, axis=1)


def own_columns(array):
    width = array.shape[1] // lax.axis_size("tp")
    return lax.dynamic_slice_in_dim(array, lax.axis_index("tp") * width, width, axis=1)


def scattered(array):
    count = lax.axis_size("tp")
    if count > 2:
        return lax.psum_scatter(array, "tp", scatter_dimension=1, tiled=True).astype(f32)
    if count == 1:
        return array.astype(f32)
    width = array.shape[1] // 2
    place = lax.axis_index("tp")
    away = lax.dynamic_slice_in_dim(array, (1 - place) * width, width, axis=1)
    here = lax.ppermute(away, "tp", [(0, 1), (1, 0)])
    return own_columns(array).astype(f32) + here.astype(f32)


def swapped(weights):
    count = lax.axis_size("inner")
    place = lax.axis_index("inner")
    rows, width = weights[0].shape[0], weights[0].shape[1] // count
    joined = [jnp.zeros((rows * count, width), w.dtype) for w in weights]
    for turn in range(count):
        there = place ^ turn
        piece = jnp.concatenate(
            [lax.dynamic_slice_in_dim(w, there * width, width, axis=1) for w in weights], axis=0
        )
        if turn:
            piece = partner(piece, turn)
        joined = [
            lax.dynamic_update_slice_in_dim(j, piece[i * rows : (i + 1) * rows], there * rows, axis=0)
            for i, j in enumerate(joined)
        ]
    return joined


def sum_tp(pair):
    if lax.axis_size("tp") == 2:
        return pair + lax.ppermute(pair, "tp", [(0, 1), (1, 0)])
    return lax.psum(pair, "tp")


def norm_scattered(added, residual, gain):
    total = resid_scale * residual.astype(f32) + added
    width = total.shape[1] * lax.axis_size("tp")
    sums = sum_tp(jnp.stack([jnp.sum(total, axis=1), jnp.sum(total * total, axis=1)]))
    mean = sums[0] / width
    variance = sums[1] / width - mean * mean
    return ((total - mean[:, None]) * lax.rsqrt(variance + norm_eps)[:, None] * gain).astype(bf16)


def spread(columns, heads_per):
    rows = columns.shape[0]
    lane = lax.broadcasted_iota(jnp.int32, (rows, 2 * HEAD_DIM), 1)
    pieces = []
    for pair in range(heads_per // 2):
        low = columns[:, 2 * pair : 2 * pair + 1]
        high = columns[:, 2 * pair + 1 : 2 * pair + 2]
        pieces.append(jnp.where(lane < HEAD_DIM, low, high))
    return jnp.concatenate(pieces, axis=1)


def mixer_kernel(
    value_ref, entry_ref, readout_ref,
    low_value_ref, low_entry_ref, low_readout_ref,
    high_value_ref, high_entry_ref, high_readout_ref,
    value_tap_ref, entry_tap_ref, readout_tap_ref,
    step_ref, sudden_ref, rate_ref, bias_ref, doc_ref, doc_row_ref,
    out_ref, readout_out_ref, far_ref, end_ref,
    window, values, entries, fresh, starts, cols, lines, sums,
):
    rows, width = value_ref.shape
    per = width // HEAD_DIM
    both = 2 * per
    blocks = rows // BLOCK
    taps = value_tap_ref.shape[0]
    half = taps // 2
    edge = 8
    pieces = [(value_ref, low_value_ref, high_value_ref, value_tap_ref, i * 128, i * 128)
              for i in range(width // 128)]
    pieces.append((entry_ref, low_entry_ref, high_entry_ref, entry_tap_ref, 0, width))
    pieces.append((readout_ref, low_readout_ref, high_readout_ref, readout_tap_ref, 0, width + 128))
    for source, low, high, _, at, to in pieces:
        window[0:edge, to : to + 128] = low[:, at : at + 128].astype(f32)
        window[edge + rows : 2 * edge + rows, to : to + 128] = high[:, at : at + 128].astype(f32)
        window[edge : edge + rows, to : to + 128] = source[:, at : at + 128].astype(f32)

    heads = step_ref.shape[1]
    head = lax.broadcasted_iota(jnp.int32, (heads, both), 0)
    lane = lax.broadcasted_iota(jnp.int32, (heads, both), 1)
    pick = head == pl.program_id(0) * per + jnp.where(lane < per, lane, lane - per)
    pick = jnp.where(pick, 1.0, 0.0)
    at = lax.broadcasted_iota(jnp.int32, (BLOCK, BLOCK), 0)
    source_at = lax.broadcasted_iota(jnp.int32, (BLOCK, BLOCK), 1)
    lower = jnp.where(at >= source_at, 1.0, 0.0)
    unit = jnp.where(at == source_at, 1.0, 0.0)
    ahead_lane = lax.broadcasted_iota(jnp.int32, (1, both), 1) < per

    def conv_block(b, _):
        start = pl.multiple_of(b * BLOCK, BLOCK)
        here = pl.ds(start, BLOCK)
        docs = doc_ref[pl.ds(start, BLOCK + 2 * edge), :]
        own = docs[edge : edge + BLOCK]
        masks = [
            jnp.where(docs[edge - half + k : edge - half + k + BLOCK] == own, 1.0, 0.0)
            for k in range(taps)
        ]
        raw = jnp.dot(step_ref[here, :].astype(f32), pick, preferred_element_type=f32)
        sudden = jnp.dot(sudden_ref[here, :], pick, precision=exact_prec, preferred_element_type=f32)
        raw = raw + bias_ref[...]
        step = jnp.maximum(raw, 0.0) + jnp.log1p(jnp.exp(-jnp.abs(raw)))
        decay = (sudden - jnp.exp(rate_ref[...]) * step) * LOG2E
        cum = jnp.dot(lower, decay, precision=exact_prec, preferred_element_type=f32)
        total = cum[BLOCK - 1 : BLOCK]
        cum = jnp.where(ahead_lane, cum, total - cum + decay)
        leave = jnp.where(ahead_lane, own[BLOCK - 1 : BLOCK], own[0:1])
        come = jnp.where(ahead_lane, docs[edge - 1 : edge], docs[edge + BLOCK : edge + BLOCK + 1])
        outward = jnp.where(own == leave, jnp.exp2(total - cum) * step, 0.0)
        arrive = jnp.where(own == come, jnp.exp2(cum), 0.0)
        passing = jnp.where(leave == come, jnp.exp2(total), 0.0)
        single = jnp.log2(step[:, :per] + step[:, per:])
        cols[here, 0:both] = cum
        cols[here, both : 2 * both] = arrive
        line = jnp.concatenate([jnp.log2(step) - cum, single, single], axis=1)
        lines[b] = lax.dot_general(
            line, unit, (((0,), (0,)), ((), ())), precision=exact_prec, preferred_element_type=f32
        )
        sums[b, 0:1, 0:both] = total
        sums[b, 1:2, 0:both] = passing
        value_parts = []
        for source, low, high, tap_ref, at, to in pieces:
            around = window[pl.ds(start, BLOCK + 2 * edge), to : to + 128]
            acc = jnp.zeros((BLOCK, 128), f32)
            for k in range(taps):
                moved = around[edge - half + k : edge - half + k + BLOCK]
                term = moved * tap_ref[k : k + 1, at : at + 128].astype(f32)
                if k != half:
                    term = term * masks[k]
                acc = acc + term
            active = 0.5 * acc * (1.0 + jnp.tanh(0.5 * acc))
            if to < width:
                value_parts.append(active)
            elif to == width:
                entry = active.astype(bf16)
            else:
                readout_out_ref[here, :] = active.astype(bf16)
        value = jnp.concatenate(value_parts, axis=1)
        values[here, :] = value.astype(bf16)
        entries[here, :] = entry
        forward = value * spread(outward[:, :per], per)
        backward = value * spread(outward[:, per:], per)
        weighted = jnp.concatenate([forward, backward], axis=1).astype(bf16)
        fresh[b] = lax.dot_general(
            entry, weighted, (((0,), (0,)), ((), ())), preferred_element_type=f32
        )
        return 0

    lax.fori_loop(0, blocks, conv_block, 0)

    prev_doc = doc_ref[edge - 1 : edge, :]
    next_doc = doc_ref[edge + rows : edge + rows + 1, :]
    first_doc = doc_ref[edge : edge + 1, :]
    last_doc = doc_ref[edge + rows - 1 : edge + rows, :]
    totals = [sums[b, 0:1, 0:both] for b in range(blocks)]
    passes = [sums[b, 1:2, 0:both] for b in range(blocks)]
    for b in range(blocks):
        nothing = jnp.zeros((1, both), f32)
        sums[b, 2:3, 0:both] = jnp.where(
            ahead_lane, sum(totals[:b], nothing), sum(totals[b + 1 :], nothing)
        )
    whole = jnp.where(
        jnp.where(ahead_lane, prev_doc, next_doc) == jnp.where(ahead_lane, last_doc, first_doc),
        jnp.exp2(sum(totals[1:], totals[0])), 0.0,
    )
    tail_row = lax.broadcasted_iota(jnp.int32, (16, width), 0)
    for k, order in ((0, range(blocks)), (1, range(blocks - 1, -1, -1))):
        span = slice(k * width, (k + 1) * width)
        state = jnp.zeros((STATE, width), f32)
        for b in order:
            starts[b, :, span] = state.astype(bf16)
            factor = spread(passes[b][:, k * per : (k + 1) * per], per)
            state = state * factor + fresh[b, :, span]
        end_ref[k, 0:STATE] = state.astype(bf16)
        factor = spread(whole[:, k * per : (k + 1) * per], per)
        coarse = factor.astype(bf16).astype(f32)
        tail = jnp.where(tail_row == 0, coarse, jnp.where(tail_row == 1, factor - coarse, 0.0))
        end_ref[k, STATE : STATE + 16] = tail.astype(bf16)

    def out_block(b, _):
        start = pl.multiple_of(b * BLOCK, BLOCK)
        here = pl.ds(start, BLOCK)
        own = doc_ref[pl.ds(start + edge, BLOCK), :]
        cum = cols[here, 0:both]
        arrive = cols[here, both : 2 * both]
        beyond = jnp.where(ahead_lane, prev_doc, next_doc)
        far_ref[here, :] = jnp.where(own == beyond, jnp.exp2(cum + sums[b, 2:3, 0:both]), 0.0)
        along = lines[b]
        readout = readout_out_ref[here, :]
        entry = entries[here, :]
        value = values[here, :]
        scores = lax.dot_general(
            readout, entry, (((1,), (1,)), ((), ())), preferred_element_type=f32
        )
        scores = jnp.where(own == doc_row_ref[b], scores, 0.0)
        at = lax.broadcasted_iota(jnp.int32, (BLOCK, BLOCK), 0)
        source_at = lax.broadcasted_iota(jnp.int32, (BLOCK, BLOCK), 1)
        value_lane = lax.broadcasted_iota(jnp.int32, (BLOCK, width), 1)
        weights = []
        spreads = []
        for r in range(per):
            ahead = cum[:, r : r + 1] + along[r : r + 1, :]
            behind = cum[:, per + r : per + r + 1] + along[per + r : per + r + 1, :]
            single = along[both + r : both + r + 1, :]
            power = jnp.where(at > source_at, ahead, jnp.where(at < source_at, behind, single))
            weights.append((scores * jnp.exp2(power)).astype(bf16))
            mine = (value_lane >= r * HEAD_DIM) & (value_lane < (r + 1) * HEAD_DIM)
            spreads.append(jnp.where(mine, value, jnp.zeros_like(value)))
        total = jnp.dot(
            jnp.concatenate(weights, axis=1),
            jnp.concatenate(spreads, axis=0),
            preferred_element_type=f32,
        )
        carried = jnp.dot(readout, starts[b], preferred_element_type=f32)
        total = total + carried[:, 0:width] * spread(arrive[:, :per], per)
        total = total + carried[:, width : 2 * width] * spread(arrive[:, per:], per)
        out_ref[here, :] = total
        return 0

    lax.fori_loop(0, blocks, out_block, 0)


def opened(packed):
    factor = packed[STATE : STATE + 1, :].astype(f32) + packed[STATE + 1 : STATE + 2, :].astype(f32)
    return packed[0:STATE, :].astype(f32), factor


def chained(earlier, later):
    return earlier[0] * later[1] + later[0], earlier[1] * later[1]


def chain_kernel(near_ahead, far_ahead, near_behind, far_behind, ahead_ref, behind_ref):
    width = near_ahead.shape[1]
    tail_row = lax.broadcasted_iota(jnp.int32, (16, width), 0)
    for near, far, out in ((near_ahead, far_ahead, ahead_ref), (near_behind, far_behind, behind_ref)):
        state, factor = chained(opened(far), opened(near))
        out[0:STATE, :] = state.astype(bf16)
        coarse = factor.astype(bf16).astype(f32)
        tail = jnp.where(tail_row == 0, coarse, jnp.where(tail_row == 1, factor - coarse, 0.0))
        out[STATE : STATE + 16, :] = tail.astype(bf16)


def gate_kernel(*refs):
    mixed_ref, readout_ref, far_ref, gate_ref, gain_ref = refs[:5]
    packs, out_ref, state_ref = refs[5:-2], refs[-2], refs[-1]
    rows, width = mixed_ref.shape
    per = width // HEAD_DIM
    count = len(packs) // 2
    for k in range(2):
        total = opened(packs[k * count])
        for pack in packs[k * count + 1 : (k + 1) * count]:
            total = chained(opened(pack), total)
        state_ref[:, k * width : (k + 1) * width] = total[0].astype(bf16)

    def one(b, _):
        here = pl.ds(pl.multiple_of(b * BLOCK, BLOCK), BLOCK)
        far = far_ref[here, :]
        carried = jnp.dot(readout_ref[here, :], state_ref[...], preferred_element_type=f32)
        total = mixed_ref[here, :]
        total = total + carried[:, 0:width] * spread(far[:, :per], per)
        total = total + carried[:, width : 2 * width] * spread(far[:, per:], per)
        gate = gate_ref[here, :].astype(f32)
        total = total * (0.5 * gate * (1.0 + jnp.tanh(0.5 * gate)))
        scale = lax.rsqrt(jnp.mean(total * total, axis=1, keepdims=True) + norm_eps)
        out_ref[here, :] = (total * scale * gain_ref[...]).astype(bf16)
        return 0

    lax.fori_loop(0, rows // BLOCK, one, 0)


def up_kernel(place_ref, own_ref, other_ref, weight_ref, out_ref):
    place = place_ref[0]
    depth = own_ref.shape[1]
    near = weight_ref[pl.ds(pl.multiple_of(place * depth, depth), depth), :]
    away = weight_ref[pl.ds(pl.multiple_of((1 - place) * depth, depth), depth), :]
    hidden = jnp.dot(own_ref[...], near, preferred_element_type=f32)
    hidden = hidden + jnp.dot(other_ref[...], away, preferred_element_type=f32)
    hidden = jnp.maximum(hidden, 0.0)
    out_ref[...] = (hidden * hidden).astype(bf16)


def up_rows(place, own, other, weight):
    rows, depth = own.shape
    units = weight.shape[1]
    tile = units // 2
    return pl.pallas_call(
        up_kernel,
        grid=(units // tile,),
        in_specs=[
            pl.BlockSpec(memory_space=pltpu.SMEM),
            pl.BlockSpec((rows, depth), lambda i: (0, 0)),
            pl.BlockSpec((rows, depth), lambda i: (0, 0)),
            pl.BlockSpec((2 * depth, tile), lambda i: (0, i)),
        ],
        out_specs=pl.BlockSpec((rows, tile), lambda i: (0, i)),
        out_shape=jax.ShapeDtypeStruct((rows, units), bf16),
        name="up_rows",
    )(place, own, other, weight)


def down_kernel(place_ref, *refs):
    pieces, (weight_ref, here_ref, away_ref) = refs[:-3], refs[-3:]
    place = place_ref[0]
    width = here_ref.shape[1]
    for which, out_ref in ((place, here_ref), (1 - place, away_ref)):
        weight = weight_ref[pl.ds(pl.multiple_of(which * width, width), width), :]
        at = 0
        for piece in pieces:
            rows = piece.shape[0]
            out_ref[at : at + rows, :] = lax.dot_general(
                piece[...], weight, (((1,), (1,)), ((), ())), preferred_element_type=f32
            ).astype(bf16)
            at += rows


def down_rows(place, pieces, weight):
    rows = sum(piece.shape[0] for piece in pieces)
    shape = jax.ShapeDtypeStruct((rows, weight.shape[0] // 2), bf16)
    vmem = pl.BlockSpec(memory_space=pltpu.VMEM)
    return pl.pallas_call(
        down_kernel,
        in_specs=[pl.BlockSpec(memory_space=pltpu.SMEM)] + [vmem] * (len(pieces) + 1),
        out_specs=[vmem, vmem],
        out_shape=[shape, shape],
        name="down_rows",
    )(place, *pieces, weight)


def norm_kernel(*refs):
    parts, (stream_ref, gain_ref, out_ref) = refs[:-3], refs[-3:]
    total = resid_scale * stream_ref[...].astype(f32)
    added = parts[0][...].astype(f32)
    for part in parts[1:]:
        added = added + part[...].astype(f32)
    total = total + added
    width = total.shape[1]
    mean = jnp.sum(total, axis=1, keepdims=True) / width
    variance = jnp.sum(total * total, axis=1, keepdims=True) / width - mean * mean
    out_ref[...] = ((total - mean) * lax.rsqrt(variance + norm_eps) * gain_ref[...]).astype(bf16)


def norm_rows(parts, stream, gain):
    rows, width = stream.shape
    tile = min(rows, BLOCK)
    spec = pl.BlockSpec((tile, width), lambda i: (i, 0))
    return pl.pallas_call(
        norm_kernel,
        grid=(rows // tile,),
        in_specs=[spec] * (len(parts) + 1) + [pl.BlockSpec((1, width), lambda i: (0, 0))],
        out_specs=spec,
        out_shape=jax.ShapeDtypeStruct((rows, width), bf16),
        name="norm_rows",
    )(*parts, stream, gain)


def per_device(
    head_value_rows,
    entry_map_rows,
    readout_map_rows,
    output_gate_rows,
    step_before_softplus,
    sudden_log_decay,
    document_index,
    head_rate_logarithm,
    head_step_bias,
    value_conv_taps,
    entry_conv_taps,
    readout_conv_taps,
    group_norm_gain,
    mixer_output_weight,
    stream,
    mixer_norm_gain,
    channel_norm_gain,
    up_projection_weight,
    down_projection_weight,
):
    up_part, down_part = swapped([up_projection_weight, down_projection_weight])
    halves = 2
    step = down_part.shape[0] // halves
    up_full = lax.all_gather(up_part, "outer", axis=0, tiled=True)
    down_full = [
        lax.all_gather(down_part[k * step : (k + 1) * step], "outer", axis=0, tiled=True)
        for k in range(halves)
    ]
    row_count = head_value_rows.shape[0]
    head_count = step_before_softplus.shape[1]
    groups = entry_map_rows.shape[1] // STATE
    per = head_count // groups
    width = per * HEAD_DIM
    blocks = row_count // BLOCK
    taps = value_conv_taps.shape[0]
    half = taps // 2
    edge = 8

    joined_low = jnp.concatenate(
        [a[-edge:] for a in (head_value_rows, entry_map_rows, readout_map_rows)], axis=1
    )
    joined_high = jnp.concatenate(
        [a[:edge] for a in (head_value_rows, entry_map_rows, readout_map_rows)], axis=1
    )
    low = shifted(joined_low, 1)
    high = shifted(joined_high, -1)

    position = lax.axis_index(SP) * row_count
    doc_pad = jnp.pad(document_index, edge, constant_values=-1)
    around = lax.dynamic_slice_in_dim(doc_pad, position, row_count + 2 * edge).astype(f32)
    doc_column = around[:, None]
    doc_rows = around[edge : edge + row_count].reshape(blocks, 1, BLOCK)

    def lanes(array):
        return array.reshape(2, groups, per).transpose(1, 0, 2).reshape(groups, 1, 2 * per)

    def rows_spec(columns_wide):
        return pl.BlockSpec((row_count, columns_wide), lambda g: (0, g))

    def thin_spec(height, columns_wide):
        return pl.BlockSpec((height, columns_wide), lambda g: (0, g))

    def group_spec(*shape):
        return pl.BlockSpec((pl.Squeezed(),) + shape, lambda g: (g,) + (0,) * len(shape))

    def same_spec(*shape):
        return pl.BlockSpec(shape, lambda g: (0,) * len(shape))

    def edge_spec(columns_wide, first):
        return pl.BlockSpec((edge, columns_wide), lambda g: (0, first // columns_wide + g))

    value_width, map_width = groups * width, groups * STATE
    edge_specs = [
        edge_spec(width, 0), edge_spec(STATE, value_width), edge_spec(STATE, value_width + map_width)
    ]
    pack_rows = STATE + 16
    local, readouts, far, ends = pl.pallas_call(
        mixer_kernel,
        grid=(groups,),
        in_specs=[
            rows_spec(width), rows_spec(STATE), rows_spec(STATE), *edge_specs, *edge_specs,
            thin_spec(taps, width), thin_spec(taps, STATE), thin_spec(taps, STATE),
            same_spec(row_count, head_count), same_spec(row_count, head_count),
            group_spec(1, 2 * per), group_spec(1, 2 * per),
            same_spec(row_count + 2 * edge, 1), same_spec(blocks, 1, BLOCK),
        ],
        out_specs=[
            rows_spec(width), rows_spec(STATE), group_spec(row_count, 2 * per),
            pl.BlockSpec((2, pl.Squeezed(), pack_rows, width), lambda g: (0, g, 0, 0)),
        ],
        out_shape=[
            jax.ShapeDtypeStruct((row_count, groups * width), f32),
            jax.ShapeDtypeStruct((row_count, groups * STATE), bf16),
            jax.ShapeDtypeStruct((groups, row_count, 2 * per), f32),
            jax.ShapeDtypeStruct((2, groups, pack_rows, width), bf16),
        ],
        scratch_shapes=[
            pltpu.VMEM((row_count + 2 * edge, width + 2 * STATE), f32),
            pltpu.VMEM((row_count, width), bf16),
            pltpu.VMEM((row_count, STATE), bf16),
            pltpu.VMEM((blocks, STATE, 2 * width), f32),
            pltpu.VMEM((blocks, STATE, 2 * width), bf16),
            pltpu.VMEM((row_count, 128), f32),
            pltpu.VMEM((blocks, 4 * per, BLOCK), f32),
            pltpu.VMEM((blocks, 8, 128), f32),
        ],
        name="mixer",
    )(
        head_value_rows, entry_map_rows, readout_map_rows, low, low, low, high, high, high,
        value_conv_taps, entry_conv_taps, readout_conv_taps,
        step_before_softplus, sudden_log_decay, lanes(head_rate_logarithm), lanes(head_step_bias),
        doc_column, doc_rows,
    )

    reach = min(lax.axis_size(SP) - 1, -(-(MAX_DOCUMENT - 1) // row_count))
    pack_spec = group_spec(pack_rows, width)
    pack_shape = jax.ShapeDtypeStruct((groups, pack_rows, width), bf16)
    firsts = [shifted(ends[k], sign * j) for k, sign in ((0, 1), (1, -1)) for j in (1, 2)]
    ahead, behind = pl.pallas_call(
        chain_kernel,
        grid=(groups,),
        in_specs=[pack_spec] * 4,
        out_specs=[pack_spec] * 2,
        out_shape=[pack_shape] * 2,
        name="chain",
    )(*firsts)
    packs = [ahead] + [shifted(ahead, j) for j in range(2, reach, 2)]
    packs = packs + [behind] + [shifted(behind, -j) for j in range(2, reach, 2)]
    normed = pl.pallas_call(
        gate_kernel,
        grid=(groups,),
        in_specs=[
            rows_spec(width), rows_spec(STATE), group_spec(row_count, 2 * per), rows_spec(width),
            thin_spec(1, width),
        ] + [pack_spec] * len(packs),
        out_specs=rows_spec(width),
        out_shape=jax.ShapeDtypeStruct((row_count, groups * width), bf16),
        scratch_shapes=[pltpu.VMEM((STATE, 2 * width), bf16)],
        name="gate",
    )(local, readouts, far, output_gate_rows, group_norm_gain[None], *packs)

    part = jnp.dot(normed, mixer_output_weight, preferred_element_type=f32).astype(bf16)
    tp_count = lax.axis_size("tp")
    if tp_count <= 2:
        stream_full = columns_over_tp(stream)
        gain_one = columns_over_tp(mixer_norm_gain[None])
        normed_one = norm_rows(over_tp(part), stream_full, gain_one)
        own_one = own_columns(normed_one)
    else:
        own_one = norm_scattered(scattered(part), stream, mixer_norm_gain)
        normed_one = columns_over_tp(own_one)

    hidden = jnp.dot(normed_one, up_full, preferred_element_type=f32)
    squared = [jnp.square(jax.nn.relu(hidden)).astype(bf16)]
    middle = row_count // 2
    beside = [partner(own_one, turn) for turn in (1, 2)]
    beside.append(partner(beside[0][:middle], 2))
    beside.append(partner(beside[1][middle:], 1))
    place = lax.axis_index("tp").astype(jnp.int32)[None]
    for rows in beside:
        if tp_count == 2:
            squared.append(up_rows(place, *over_tp(rows), up_full))
        else:
            hidden = jnp.dot(columns_over_tp(rows), up_full, preferred_element_type=f32)
            squared.append(jnp.square(jax.nn.relu(hidden)).astype(bf16))

    def add_rounded(left, right):
        return (left.astype(f32) + right.astype(f32)).astype(bf16)

    sums = []
    for weight in down_full:
        if tp_count == 2:
            here, away = down_rows(place, squared, weight)
            total = add_rounded(here, over_tp(away)[1])
        else:
            product = lax.dot_general(
                jnp.concatenate(squared, axis=0), weight, (((1,), (1,)), ((), ())),
                preferred_element_type=f32,
            )
            total = scattered(product.astype(bf16)).astype(bf16)
        own, by_x, by_y, by_both = jnp.split(total, 4, axis=0)
        for_x = partner(by_both[:middle], 2)
        for_y = partner(by_both[middle:], 1)
        by_x = jnp.concatenate([add_rounded(by_x[:middle], for_x), by_x[middle:]], axis=0)
        by_y = jnp.concatenate([by_y[:middle], add_rounded(by_y[middle:], for_y)], axis=0)
        sums.append(own.astype(f32) + partner(by_x, 1).astype(f32) + partner(by_y, 2).astype(f32))
    strips = lax.axis_size("outer") // tp_count
    added = jnp.concatenate(
        [jnp.split(total, strips, axis=1)[strip] for strip in range(strips) for total in sums], axis=1
    )
    return norm_scattered(added, own_one, channel_norm_gain)


def solution(mesh):
    sp_count, tp_count = mesh.devices.shape
    inner = 4
    finer = jax.sharding.Mesh(
        mesh.devices.reshape(sp_count // inner, inner, tp_count), ("outer", "inner", "tp")
    )
    both = P(SP, "tp")
    second = P(None, "tp")
    placed = (
        both, both, both, both, both, both, P(), second, second, second, second, second,
        P("tp"), P("tp", None), both, P("tp"), P("tp"), both, both,
    )
    return jax.shard_map(
        per_device, mesh=finer, in_specs=placed, out_specs=both, check_vma=False
    )
```

```python
import functools

import jax
import jax.numpy as jnp
from jax import lax
from jax.experimental import pallas as pl
from jax.experimental.pallas import tpu as pltpu
from jax.sharding import PartitionSpec as P


HEAD_DIM = 64
STATE = 128
BLOCK = 128
MAX_DOCUMENT = 6144
LOG2E = 1.4426950408889634
SIDE = 4

exact_prec = lax.Precision.HIGHEST
norm_eps = 1e-05
resid_scale = 1.4142135623730951
f32 = jnp.float32
bf16 = jnp.bfloat16


SP = ("outer", "inner")


def shifted(array, by, axis=SP):
    count = lax.axis_size(axis)
    pairs = [(i, i + by) for i in range(count) if 0 <= i + by < count]
    return lax.ppermute(array, axis, pairs)


def together(*trees):
    return lax.optimization_barrier(trees)


def partner(array, turn):
    return lax.ppermute(array, "inner", [(i, i ^ turn) for i in range(lax.axis_size("inner"))])


def over_tp(array):
    count = lax.axis_size("tp")
    if count == 1:
        return [array]
    return [array, lax.ppermute(array, "tp", [(0, 1), (1, 0)])]


def columns_over_tp(array):
    count = lax.axis_size("tp")
    if count == 1:
        return array
    if count > 2:
        return lax.all_gather(array, "tp", axis=1, tiled=True)
    own, other = over_tp(array)
    width = array.shape[1]
    place = lax.axis_index("tp")
    joined = jnp.zeros((array.shape[0], 2 * width), array.dtype)
    joined = lax.dynamic_update_slice_in_dim(joined, own, place * width, axis=1)
    return lax.dynamic_update_slice_in_dim(joined, other, (1 - place) * width, axis=1)


def own_columns(array):
    width = array.shape[1] // lax.axis_size("tp")
    return lax.dynamic_slice_in_dim(array, lax.axis_index("tp") * width, width, axis=1)


def scattered(array):
    count = lax.axis_size("tp")
    if count > 2:
        return lax.psum_scatter(array, "tp", scatter_dimension=1, tiled=True).astype(f32)
    if count == 1:
        return array.astype(f32)
    width = array.shape[1] // 2
    place = lax.axis_index("tp")
    away = lax.dynamic_slice_in_dim(array, (1 - place) * width, width, axis=1)
    here = lax.ppermute(away, "tp", [(0, 1), (1, 0)])
    return own_columns(array).astype(f32) + here.astype(f32)


def swap_start(weight):
    count = lax.axis_size("inner")
    place = lax.axis_index("inner")
    width = weight.shape[1] // count
    pieces = []
    for turn in range(count):
        piece = lax.dynamic_slice_in_dim(weight, (place ^ turn) * width, width, axis=1)
        pieces.append(partner(piece, turn) if turn else piece)
    return pieces


def swap_finish(pieces):
    place = lax.axis_index("inner")
    rows, width = pieces[0].shape
    joined = jnp.zeros((rows * len(pieces), width), pieces[0].dtype)
    for turn, piece in enumerate(pieces):
        joined = lax.dynamic_update_slice_in_dim(joined, piece, (place ^ turn) * rows, axis=0)
    return joined


def sum_tp(pair):
    if lax.axis_size("tp") == 2:
        return pair + lax.ppermute(pair, "tp", [(0, 1), (1, 0)])
    return lax.psum(pair, "tp")


def norm_scattered(added, residual, gain):
    total = resid_scale * residual.astype(f32) + added
    width = total.shape[1] * lax.axis_size("tp")
    sums = sum_tp(jnp.stack([jnp.sum(total, axis=1), jnp.sum(total * total, axis=1)]))
    mean = sums[0] / width
    variance = sums[1] / width - mean * mean
    return ((total - mean[:, None]) * lax.rsqrt(variance + norm_eps)[:, None] * gain).astype(bf16)


def spread(columns, heads_per):
    rows = columns.shape[0]
    lane = lax.broadcasted_iota(jnp.int32, (rows, 2 * HEAD_DIM), 1)
    pieces = []
    for pair in range(heads_per // 2):
        low = columns[:, 2 * pair : 2 * pair + 1]
        high = columns[:, 2 * pair + 1 : 2 * pair + 2]
        pieces.append(jnp.where(lane < HEAD_DIM, low, high))
    return jnp.concatenate(pieces, axis=1)


def mixer_kernel(
    value_ref, entry_ref, readout_ref,
    low_value_ref, low_entry_ref, low_readout_ref,
    high_value_ref, high_entry_ref, high_readout_ref,
    value_tap_ref, entry_tap_ref, readout_tap_ref,
    step_ref, sudden_ref, rate_ref, bias_ref, doc_ref, doc_row_ref, *rest,
    first_group,
):
    (out_ref, readout_out_ref, far_ref, end_ref,
     window, values, entries, fresh, starts, cols, lines, sums) = rest[-12:]
    rows, width = value_ref.shape
    per = width // HEAD_DIM
    both = 2 * per
    blocks = rows // BLOCK
    taps = value_tap_ref.shape[0]
    half = taps // 2
    edge = 8
    pieces = [(value_ref, low_value_ref, high_value_ref, value_tap_ref, i * 128, i * 128)
              for i in range(width // 128)]
    pieces.append((entry_ref, low_entry_ref, high_entry_ref, entry_tap_ref, 0, width))
    pieces.append((readout_ref, low_readout_ref, high_readout_ref, readout_tap_ref, 0, width + 128))
    for source, low, high, _, at, to in pieces:
        window[0:edge, to : to + 128] = low[:, at : at + 128].astype(f32)
        window[edge + rows : 2 * edge + rows, to : to + 128] = high[:, at : at + 128].astype(f32)
        window[edge : edge + rows, to : to + 128] = source[:, at : at + 128].astype(f32)

    heads = step_ref.shape[1]
    head = lax.broadcasted_iota(jnp.int32, (heads, both), 0)
    lane = lax.broadcasted_iota(jnp.int32, (heads, both), 1)
    pick = head == (first_group + pl.program_id(0)) * per + jnp.where(lane < per, lane, lane - per)
    pick = jnp.where(pick, 1.0, 0.0)
    at = lax.broadcasted_iota(jnp.int32, (BLOCK, BLOCK), 0)
    source_at = lax.broadcasted_iota(jnp.int32, (BLOCK, BLOCK), 1)
    lower = jnp.where(at >= source_at, 1.0, 0.0)
    unit = jnp.where(at == source_at, 1.0, 0.0)
    ahead_lane = lax.broadcasted_iota(jnp.int32, (1, both), 1) < per

    def conv_block(b, _):
        start = pl.multiple_of(b * BLOCK, BLOCK)
        here = pl.ds(start, BLOCK)
        docs = doc_ref[pl.ds(start, BLOCK + 2 * edge), :]
        own = docs[edge : edge + BLOCK]
        masks = [
            jnp.where(docs[edge - half + k : edge - half + k + BLOCK] == own, 1.0, 0.0)
            for k in range(taps)
        ]
        raw = jnp.dot(step_ref[here, :].astype(f32), pick, preferred_element_type=f32)
        sudden = jnp.dot(sudden_ref[here, :], pick, precision=exact_prec, preferred_element_type=f32)
        raw = raw + bias_ref[...]
        step = jnp.maximum(raw, 0.0) + jnp.log1p(jnp.exp(-jnp.abs(raw)))
        decay = (sudden - jnp.exp(rate_ref[...]) * step) * LOG2E
        cum = jnp.dot(lower, decay, precision=exact_prec, preferred_element_type=f32)
        total = cum[BLOCK - 1 : BLOCK]
        cum = jnp.where(ahead_lane, cum, total - cum + decay)
        leave = jnp.where(ahead_lane, own[BLOCK - 1 : BLOCK], own[0:1])
        come = jnp.where(ahead_lane, docs[edge - 1 : edge], docs[edge + BLOCK : edge + BLOCK + 1])
        outward = jnp.where(own == leave, jnp.exp2(total - cum) * step, 0.0)
        arrive = jnp.where(own == come, jnp.exp2(cum), 0.0)
        passing = jnp.where(leave == come, jnp.exp2(total), 0.0)
        single = jnp.log2(step[:, :per] + step[:, per:])
        cols[here, 0:both] = cum
        cols[here, both : 2 * both] = arrive
        line = jnp.concatenate([jnp.log2(step) - cum, single, single], axis=1)
        lines[b] = lax.dot_general(
            line, unit, (((0,), (0,)), ((), ())), precision=exact_prec, preferred_element_type=f32
        )
        sums[b, 0:1, 0:both] = total
        sums[b, 1:2, 0:both] = passing
        value_parts = []
        for source, low, high, tap_ref, at, to in pieces:
            around = window[pl.ds(start, BLOCK + 2 * edge), to : to + 128]
            acc = jnp.zeros((BLOCK, 128), f32)
            for k in range(taps):
                moved = around[edge - half + k : edge - half + k + BLOCK]
                term = moved * tap_ref[k : k + 1, at : at + 128].astype(f32)
                if k != half:
                    term = term * masks[k]
                acc = acc + term
            active = 0.5 * acc * (1.0 + jnp.tanh(0.5 * acc))
            if to < width:
                value_parts.append(active)
            elif to == width:
                entry = active.astype(bf16)
            else:
                readout_out_ref[here, :] = active.astype(bf16)
        value = jnp.concatenate(value_parts, axis=1)
        values[here, :] = value.astype(bf16)
        entries[here, :] = entry
        forward = value * spread(outward[:, :per], per)
        backward = value * spread(outward[:, per:], per)
        weighted = jnp.concatenate([forward, backward], axis=1).astype(bf16)
        fresh[b] = lax.dot_general(
            entry, weighted, (((0,), (0,)), ((), ())), preferred_element_type=f32
        )
        return 0

    lax.fori_loop(0, blocks, conv_block, 0)

    prev_doc = doc_ref[edge - 1 : edge, :]
    next_doc = doc_ref[edge + rows : edge + rows + 1, :]
    first_doc = doc_ref[edge : edge + 1, :]
    last_doc = doc_ref[edge + rows - 1 : edge + rows, :]
    totals = [sums[b, 0:1, 0:both] for b in range(blocks)]
    passes = [sums[b, 1:2, 0:both] for b in range(blocks)]
    for b in range(blocks):
        nothing = jnp.zeros((1, both), f32)
        sums[b, 2:3, 0:both] = jnp.where(
            ahead_lane, sum(totals[:b], nothing), sum(totals[b + 1 :], nothing)
        )
    whole = jnp.where(
        jnp.where(ahead_lane, prev_doc, next_doc) == jnp.where(ahead_lane, last_doc, first_doc),
        jnp.exp2(sum(totals[1:], totals[0])), 0.0,
    )
    tail_row = lax.broadcasted_iota(jnp.int32, (16, width), 0)
    for k, order in ((0, range(blocks)), (1, range(blocks - 1, -1, -1))):
        span = slice(k * width, (k + 1) * width)
        state = jnp.zeros((STATE, width), f32)
        for b in order:
            starts[b, :, span] = state.astype(bf16)
            factor = spread(passes[b][:, k * per : (k + 1) * per], per)
            state = state * factor + fresh[b, :, span]
        share = STATE // SIDE
        for q in range(SIDE):
            end_ref[q, k, 0:share] = state[q * share : (q + 1) * share].astype(bf16)
        factor = spread(whole[:, k * per : (k + 1) * per], per)
        coarse = factor.astype(bf16).astype(f32)
        tail = jnp.where(tail_row == 0, coarse, jnp.where(tail_row == 1, factor - coarse, 0.0))
        for q in range(SIDE):
            end_ref[q, k, share : share + 16] = tail.astype(bf16)

    def out_block(b, _):
        start = pl.multiple_of(b * BLOCK, BLOCK)
        here = pl.ds(start, BLOCK)
        own = doc_ref[pl.ds(start + edge, BLOCK), :]
        cum = cols[here, 0:both]
        arrive = cols[here, both : 2 * both]
        beyond = jnp.where(ahead_lane, prev_doc, next_doc)
        far_ref[here, :] = jnp.where(own == beyond, jnp.exp2(cum + sums[b, 2:3, 0:both]), 0.0)
        along = lines[b]
        readout = readout_out_ref[here, :]
        entry = entries[here, :]
        value = values[here, :]
        scores = lax.dot_general(
            readout, entry, (((1,), (1,)), ((), ())), preferred_element_type=f32
        )
        scores = jnp.where(own == doc_row_ref[b], scores, 0.0)
        at = lax.broadcasted_iota(jnp.int32, (BLOCK, BLOCK), 0)
        source_at = lax.broadcasted_iota(jnp.int32, (BLOCK, BLOCK), 1)
        value_lane = lax.broadcasted_iota(jnp.int32, (BLOCK, width), 1)
        weights = []
        spreads = []
        for r in range(per):
            ahead = cum[:, r : r + 1] + along[r : r + 1, :]
            behind = cum[:, per + r : per + r + 1] + along[per + r : per + r + 1, :]
            single = along[both + r : both + r + 1, :]
            power = jnp.where(at > source_at, ahead, jnp.where(at < source_at, behind, single))
            weights.append((scores * jnp.exp2(power)).astype(bf16))
            mine = (value_lane >= r * HEAD_DIM) & (value_lane < (r + 1) * HEAD_DIM)
            spreads.append(jnp.where(mine, value, jnp.zeros_like(value)))
        total = jnp.dot(
            jnp.concatenate(weights, axis=1),
            jnp.concatenate(spreads, axis=0),
            preferred_element_type=f32,
        )
        carried = jnp.dot(readout, starts[b], preferred_element_type=f32)
        total = total + carried[:, 0:width] * spread(arrive[:, :per], per)
        total = total + carried[:, width : 2 * width] * spread(arrive[:, per:], per)
        out_ref[here, :] = total
        return 0

    lax.fori_loop(0, blocks, out_block, 0)


def opened(packed):
    rows = packed.shape[0] - 16
    factor = packed[rows : rows + 1, :].astype(f32) + packed[rows + 1 : rows + 2, :].astype(f32)
    return packed[0:rows, :].astype(f32), factor


def closed(pair):
    state, factor = pair
    tail_row = lax.broadcasted_iota(jnp.int32, (16, state.shape[1]), 0)
    coarse = factor.astype(bf16).astype(f32)
    tail = jnp.where(tail_row == 0, coarse, jnp.where(tail_row == 1, factor - coarse, 0.0))
    return jnp.concatenate([state, tail], axis=0).astype(bf16)


def chained(earlier, later):
    return earlier[0] * later[1] + later[0], earlier[1] * later[1]


def whole_kernel(place_ref, *refs):
    pieces, (ahead_ref, behind_ref, ordered) = refs[:-3], refs[-3:]
    for turn, piece in enumerate(pieces):
        ordered[place_ref[0] ^ turn] = piece[...]
    for k, order, out in ((0, (1, 2, 3), ahead_ref), (1, (2, 1, 0), behind_ref)):
        total = opened(ordered[0 if k == 0 else SIDE - 1, k])
        for j in order:
            total = chained(total, opened(ordered[j, k]))
        out[...] = closed(total)


def arrive_kernel(place_ref, *refs):
    pieces, others, (out_ref, ordered, arrived) = refs[:SIDE], refs[SIDE:-3], refs[-3:]
    for turn, piece in enumerate(pieces):
        ordered[place_ref[0] ^ turn] = piece[...]
    count = len(others) // 2
    width = pieces[0].shape[2]
    for k, order in ((0, range(SIDE)), (1, range(SIDE - 1, -1, -1))):
        total = opened(others[k * count])
        for other in others[k * count + 1 : (k + 1) * count]:
            total = chained(opened(other), total)
        for j in order:
            arrived[j, :, k * width : (k + 1) * width] = total[0].astype(bf16)
            total = chained(total, opened(ordered[j, k]))
    for turn in range(SIDE):
        out_ref[turn] = arrived[place_ref[0] ^ turn]


def gate_kernel(place_ref, *refs):
    mixed_ref, readout_ref, far_ref, gate_ref, gain_ref = refs[:5]
    pieces, out_ref, state_ref = refs[5:-2], refs[-2], refs[-1]
    rows, width = mixed_ref.shape
    per = width // HEAD_DIM
    share = STATE // SIDE
    for turn, piece in enumerate(pieces):
        at = pl.multiple_of((place_ref[0] ^ turn) * share, share)
        state_ref[pl.ds(at, share), :] = piece[...]

    def one(b, _):
        here = pl.ds(pl.multiple_of(b * BLOCK, BLOCK), BLOCK)
        far = far_ref[here, :]
        carried = jnp.dot(readout_ref[here, :], state_ref[...], preferred_element_type=f32)
        total = mixed_ref[here, :]
        total = total + carried[:, 0:width] * spread(far[:, :per], per)
        total = total + carried[:, width : 2 * width] * spread(far[:, per:], per)
        gate = gate_ref[here, :].astype(f32)
        total = total * (0.5 * gate * (1.0 + jnp.tanh(0.5 * gate)))
        scale = lax.rsqrt(jnp.mean(total * total, axis=1, keepdims=True) + norm_eps)
        out_ref[here, :] = (total * scale * gain_ref[...]).astype(bf16)
        return 0

    lax.fori_loop(0, rows // BLOCK, one, 0)


def up_kernel(place_ref, own_ref, other_ref, weight_ref, out_ref, rows_ref):
    depth = own_ref.shape[1]
    outer, wide, tile = weight_ref.shape

    @pl.when(pl.program_id(0) == 0)
    def _():
        place = place_ref[0]
        rows_ref[:, pl.ds(pl.multiple_of(place * depth, depth), depth)] = own_ref[...]
        rows_ref[:, pl.ds(pl.multiple_of((1 - place) * depth, depth), depth)] = other_ref[...]

    weight = weight_ref[...].reshape(outer * wide, tile)
    hidden = jnp.dot(rows_ref[...], weight, preferred_element_type=f32)
    hidden = jnp.maximum(hidden, 0.0)
    out_ref[...] = (hidden * hidden).astype(bf16)


def up_rows(place, own, other, weights):
    rows, depth = own.shape
    outer, wide, units = weights.shape
    tile = units // 2
    return pl.pallas_call(
        up_kernel,
        grid=(units // tile,),
        in_specs=[
            pl.BlockSpec(memory_space=pltpu.SMEM),
            pl.BlockSpec((rows, depth), lambda i: (0, 0)),
            pl.BlockSpec((rows, depth), lambda i: (0, 0)),
            pl.BlockSpec((outer, wide, tile), lambda i: (0, 0, i)),
        ],
        out_specs=pl.BlockSpec((rows, tile), lambda i: (0, i)),
        out_shape=jax.ShapeDtypeStruct((rows, units), bf16),
        scratch_shapes=[pltpu.VMEM((rows, 2 * depth), bf16)],
        name="up_rows",
    )(place, own, other, weights)


def down_kernel(place_ref, *refs):
    pieces, (weight_ref, out_ref) = refs[:-2], refs[-2:]
    at = 0
    for piece in pieces:
        rows = piece.shape[0]
        out_ref[at : at + rows, :] = lax.dot_general(
            piece[...], weight_ref[...], (((1,), (1,)), ((), ())), preferred_element_type=f32
        ).astype(bf16)
        at += rows


def down_rows(place, pieces, weights):
    rows = sum(piece.shape[0] for piece in pieces)
    outer, wide, units = weights.shape
    half = outer // 2
    grid_spec = pltpu.PrefetchScalarGridSpec(
        num_scalar_prefetch=1,
        grid=(outer,),
        in_specs=[pl.BlockSpec(piece.shape, lambda i, place: (0, 0)) for piece in pieces] + [
            pl.BlockSpec(
                (pl.Squeezed(), wide, units),
                lambda i, place: ((i + place[0] * half) % outer, 0, 0),
            )
        ],
        out_specs=pl.BlockSpec(
            (pl.Squeezed(), rows, wide), lambda i, place: (i // half, 0, i % half)
        ),
    )
    return pl.pallas_call(
        down_kernel,
        grid_spec=grid_spec,
        out_shape=jax.ShapeDtypeStruct((2, rows, half * wide), bf16),
        name="down_rows",
    )(place, *pieces, weights)


def norm_kernel(place_ref, *refs):
    parts, (stream_ref, gain_ref, own_ref, other_ref) = refs[:-4], refs[-4:]
    total = resid_scale * stream_ref[...].astype(f32)
    added = parts[0][...].astype(f32)
    for part in parts[1:]:
        added = added + part[...].astype(f32)
    total = total + added
    width = total.shape[1]
    mean = jnp.sum(total, axis=1, keepdims=True) / width
    variance = jnp.sum(total * total, axis=1, keepdims=True) / width - mean * mean
    normed = (total - mean) * lax.rsqrt(variance + norm_eps) * gain_ref[...]
    left, right = normed[:, : width // 2], normed[:, width // 2 :]
    first = place_ref[0] == 0
    own_ref[...] = jnp.where(first, left, right).astype(bf16)
    other_ref[...] = jnp.where(first, right, left).astype(bf16)


def norm_rows(place, parts, stream, gain):
    rows, width = stream.shape
    tile = min(rows, BLOCK)
    spec = pl.BlockSpec((tile, width), lambda i: (i, 0))
    half_spec = pl.BlockSpec((tile, width // 2), lambda i: (i, 0))
    return pl.pallas_call(
        norm_kernel,
        grid=(rows // tile,),
        in_specs=[pl.BlockSpec(memory_space=pltpu.SMEM)] + [spec] * (len(parts) + 1)
        + [pl.BlockSpec((1, width), lambda i: (0, 0))],
        out_specs=[half_spec] * 2,
        out_shape=[jax.ShapeDtypeStruct((rows, width // 2), bf16)] * 2,
        name="norm_rows",
    )(place, *parts, stream, gain)


def per_device(
    head_value_rows,
    entry_map_rows,
    readout_map_rows,
    output_gate_rows,
    step_before_softplus,
    sudden_log_decay,
    document_index,
    head_rate_logarithm,
    head_step_bias,
    value_conv_taps,
    entry_conv_taps,
    readout_conv_taps,
    group_norm_gain,
    mixer_output_weight,
    stream,
    mixer_norm_gain,
    channel_norm_gain,
    up_projection_weight,
    down_projection_weight,
):
    row_count = head_value_rows.shape[0]
    head_count = step_before_softplus.shape[1]
    groups = entry_map_rows.shape[1] // STATE
    per = head_count // groups
    width = per * HEAD_DIM
    blocks = row_count // BLOCK
    taps = value_conv_taps.shape[0]
    edge = 8

    joined_low = jnp.concatenate(
        [a[-edge:] for a in (head_value_rows, entry_map_rows, readout_map_rows)], axis=1
    )
    joined_high = jnp.concatenate(
        [a[:edge] for a in (head_value_rows, entry_map_rows, readout_map_rows)], axis=1
    )
    low = shifted(joined_low, 1)
    high = shifted(joined_high, -1)
    up_swaps = swap_start(up_projection_weight)
    (low, high), up_swaps, down_own = together((low, high), up_swaps, down_projection_weight)
    up_weights = lax.all_gather(swap_finish(up_swaps), "outer")
    down_swaps = swap_start(down_own)

    position = lax.axis_index(SP) * row_count
    doc_pad = jnp.pad(document_index, edge, constant_values=-1)
    around = lax.dynamic_slice_in_dim(doc_pad, position, row_count + 2 * edge).astype(f32)
    doc_column = around[:, None]
    doc_rows = around[edge : edge + row_count].reshape(blocks, 1, BLOCK)

    def lanes(array):
        return array.reshape(2, groups, per).transpose(1, 0, 2).reshape(groups, 1, 2 * per)

    def rows_spec(columns_wide, first=0):
        return pl.BlockSpec((row_count, columns_wide), lambda g: (0, first + g))

    def thin_spec(height, columns_wide, first=0):
        return pl.BlockSpec((height, columns_wide), lambda g: (0, first + g))

    def group_spec(*shape, first=0):
        return pl.BlockSpec(
            (pl.Squeezed(),) + shape, lambda g: (first + g,) + (0,) * len(shape)
        )

    def same_spec(*shape):
        return pl.BlockSpec(shape, lambda g: (0,) * len(shape))

    value_width, map_width = groups * width, groups * STATE
    share = STATE // SIDE
    pack_rows = share + 16

    def mixer(first, count, so_far):
        edge_specs = [
            thin_spec(edge, width, first),
            thin_spec(edge, STATE, value_width // STATE + first),
            thin_spec(edge, STATE, (value_width + map_width) // STATE + first),
        ]
        given = [
            head_value_rows, entry_map_rows, readout_map_rows, low, low, low, high, high, high,
            value_conv_taps, entry_conv_taps, readout_conv_taps, step_before_softplus,
            sudden_log_decay, lanes(head_rate_logarithm), lanes(head_step_bias), doc_column, doc_rows,
        ]
        return pl.pallas_call(
            functools.partial(mixer_kernel, first_group=first),
            grid=(count,),
            in_specs=[
                rows_spec(width, first), rows_spec(STATE, first), rows_spec(STATE, first),
                *edge_specs, *edge_specs,
                thin_spec(taps, width, first), thin_spec(taps, STATE, first),
                thin_spec(taps, STATE, first),
                same_spec(row_count, head_count), same_spec(row_count, head_count),
                group_spec(1, 2 * per, first=first), group_spec(1, 2 * per, first=first),
                same_spec(row_count + 2 * edge, 1), same_spec(blocks, 1, BLOCK),
            ] + [pl.BlockSpec(memory_space=pl.ANY)] * len(so_far),
            out_specs=[
                rows_spec(width, first), rows_spec(STATE, first),
                group_spec(row_count, 2 * per, first=first),
                pl.BlockSpec(
                    (SIDE, 2, pl.Squeezed(), pack_rows, width), lambda g: (0, 0, first + g, 0, 0)
                ),
            ],
            out_shape=[
                jax.ShapeDtypeStruct((row_count, groups * width), f32),
                jax.ShapeDtypeStruct((row_count, groups * STATE), bf16),
                jax.ShapeDtypeStruct((groups, row_count, 2 * per), f32),
                jax.ShapeDtypeStruct((SIDE, 2, groups, pack_rows, width), bf16),
            ],
            input_output_aliases={len(given) + i: i for i in range(len(so_far))},
            scratch_shapes=[
                pltpu.VMEM((row_count + 2 * edge, width + 2 * STATE), f32),
                pltpu.VMEM((row_count, width), bf16),
                pltpu.VMEM((row_count, STATE), bf16),
                pltpu.VMEM((blocks, STATE, 2 * width), f32),
                pltpu.VMEM((blocks, STATE, 2 * width), bf16),
                pltpu.VMEM((row_count, 128), f32),
                pltpu.VMEM((blocks, 4 * per, BLOCK), f32),
                pltpu.VMEM((blocks, 8, 128), f32),
            ],
            name="mixer",
        )(*given, *so_far)

    local, readouts, far, ends = mixer(0, groups, [])

    reach = min(lax.axis_size(SP) - 1, -(-(MAX_DOCUMENT - 1) // row_count))
    spans = -(-reach // SIDE)
    inner_place = lax.axis_index("inner").astype(jnp.int32)[None]

    def share_of(array, turn):
        return lax.dynamic_index_in_dim(array, lax.axis_index("inner") ^ turn, 0, keepdims=False)

    shares = [share_of(ends, 0)] + [partner(share_of(ends, turn), turn) for turn in (1, 2, 3)]
    smem = pl.BlockSpec(memory_space=pltpu.SMEM)
    share_spec = pl.BlockSpec((2, pl.Squeezed(), pack_rows, width), lambda g: (0, g, 0, 0))
    pack_spec = group_spec(pack_rows, width)
    pack_shape = jax.ShapeDtypeStruct((groups, pack_rows, width), bf16)
    ordered = pltpu.VMEM((SIDE, 2, pack_rows, width), bf16)
    ahead, behind = pl.pallas_call(
        whole_kernel,
        grid=(groups,),
        in_specs=[smem] + [share_spec] * SIDE,
        out_specs=[pack_spec] * 2,
        out_shape=[pack_shape] * 2,
        scratch_shapes=[ordered],
        name="whole",
    )(inner_place, *shares)
    others = [shifted(ahead, j, "outer") for j in range(1, spans + 1)]
    others = others + [shifted(behind, -j, "outer") for j in range(1, spans + 1)]
    arrivals = pl.pallas_call(
        arrive_kernel,
        grid=(groups,),
        in_specs=[smem] + [share_spec] * SIDE + [pack_spec] * len(others),
        out_specs=pl.BlockSpec((SIDE, pl.Squeezed(), share, 2 * width), lambda g: (0, g, 0, 0)),
        out_shape=jax.ShapeDtypeStruct((SIDE, groups, share, 2 * width), bf16),
        scratch_shapes=[ordered, pltpu.VMEM((SIDE, share, 2 * width), bf16)],
        name="arrive",
    )(inner_place, *shares, *others)
    packs = [arrivals[0]] + [partner(arrivals[turn], turn) for turn in (1, 2, 3)]
    down_weights = lax.all_gather(swap_finish(down_swaps), "outer")

    tp_count = lax.axis_size("tp")
    if tp_count == 2:
        stream_full = columns_over_tp(stream)
        gain_one = columns_over_tp(mixer_norm_gain[None])
        packs, stream_full, gain_one = together(packs, stream_full, gain_one)
    normed = pl.pallas_call(
        gate_kernel,
        grid=(groups,),
        in_specs=[
            smem, rows_spec(width), rows_spec(STATE), group_spec(row_count, 2 * per),
            rows_spec(width), thin_spec(1, width),
        ] + [group_spec(share, 2 * width)] * SIDE,
        out_specs=rows_spec(width),
        out_shape=jax.ShapeDtypeStruct((row_count, groups * width), bf16),
        scratch_shapes=[pltpu.VMEM((STATE, 2 * width), bf16)],
        name="gate",
    )(inner_place, local, readouts, far, output_gate_rows, group_norm_gain[None], *packs)

    part = jnp.dot(normed, mixer_output_weight, preferred_element_type=f32).astype(bf16)
    place = lax.axis_index("tp").astype(jnp.int32)[None]
    if tp_count == 2:
        own_one, other_one = norm_rows(place, over_tp(part), stream_full, gain_one)
    else:
        own_one = norm_scattered(scattered(part), stream, mixer_norm_gain)
        other_one = None

    def hidden_units(rows, other=None):
        if tp_count == 2:
            other = over_tp(rows)[1] if other is None else other
            return up_rows(place, rows, other, up_weights)
        up = up_weights.reshape(-1, up_weights.shape[2])
        hidden = jnp.dot(columns_over_tp(rows), up, preferred_element_type=f32)
        return jnp.square(jax.nn.relu(hidden)).astype(bf16)

    def contributions(pieces):
        if tp_count == 2:
            both = down_rows(place, pieces, down_weights)
            other = lax.ppermute(both[1], "tp", [(0, 1), (1, 0)])
            return (both[0].astype(f32) + other.astype(f32)).astype(bf16)
        down = down_weights.reshape(-1, down_weights.shape[2])
        product = lax.dot_general(
            jnp.concatenate(pieces, axis=0), down, (((1,), (1,)), ((), ())),
            preferred_element_type=f32,
        )
        return scattered(product.astype(bf16)).astype(bf16)

    middle = row_count // 2
    side_one, side_two = partner(own_one, 1), partner(own_one, 2)
    units = hidden_units(own_one, other_one)
    side_one, side_two, units = together(side_one, side_two, units)
    far_one = partner(side_one[:middle], 2)
    far_two = partner(side_two[middle:], 1)
    near_units = [units, hidden_units(side_one), hidden_units(side_two)]
    near = contributions(near_units)
    far_rows = [far_one, far_two]
    near, far_rows = together(near, far_rows)
    back_one = partner(near[row_count : 2 * row_count], 1)
    back_two = partner(near[2 * row_count :], 2)
    diagonal_units = [hidden_units(rows) for rows in far_rows]
    diagonal = contributions(diagonal_units)
    first_hop = [partner(diagonal[:middle], 2), partner(diagonal[middle:], 1)]
    second_hop = [partner(first_hop[0], 1), partner(first_hop[1], 2)]
    added = near[:row_count].astype(f32) + back_one.astype(f32) + back_two.astype(f32)
    added = added + jnp.concatenate(second_hop, axis=0).astype(f32)
    return norm_scattered(added, own_one, channel_norm_gain)


def solution(mesh):
    sp_count, tp_count = mesh.devices.shape
    inner = SIDE
    finer = jax.sharding.Mesh(
        mesh.devices.reshape(sp_count // inner, inner, tp_count), ("outer", "inner", "tp")
    )
    both = P(SP, "tp")
    second = P(None, "tp")
    placed = (
        both, both, both, both, both, both, P(), second, second, second, second, second,
        P("tp"), P("tp", None), both, P("tp"), P("tp"), both, both,
    )
    return jax.shard_map(
        per_device, mesh=finer, in_specs=placed, out_specs=both, check_vma=False
    )
```

```python
import functools

import jax
import jax.numpy as jnp
from jax import lax
from jax.experimental import pallas as pl
from jax.experimental.pallas import tpu as pltpu
from jax.sharding import PartitionSpec as P


HEAD_DIM = 64
STATE = 128
BLOCK = 128
MAX_DOCUMENT = 6144
LOG2E = 1.4426950408889634
SIDE = 4

exact_prec = lax.Precision.HIGHEST
norm_eps = 1e-05
resid_scale = 1.4142135623730951
f32 = jnp.float32
bf16 = jnp.bfloat16


SP = ("outer", "inner")


def shifted(array, by, axis=SP):
    count = lax.axis_size(axis)
    pairs = [(i, i + by) for i in range(count) if 0 <= i + by < count]
    return lax.ppermute(array, axis, pairs)


def together(*trees):
    return lax.optimization_barrier(trees)


def partner(array, turn):
    return lax.ppermute(array, "inner", [(i, i ^ turn) for i in range(lax.axis_size("inner"))])


def over_tp(array):
    count = lax.axis_size("tp")
    if count == 1:
        return [array]
    return [array, lax.ppermute(array, "tp", [(0, 1), (1, 0)])]


def columns_over_tp(array):
    count = lax.axis_size("tp")
    if count == 1:
        return array
    if count > 2:
        return lax.all_gather(array, "tp", axis=1, tiled=True)
    own, other = over_tp(array)
    width = array.shape[1]
    place = lax.axis_index("tp")
    joined = jnp.zeros((array.shape[0], 2 * width), array.dtype)
    joined = lax.dynamic_update_slice_in_dim(joined, own, place * width, axis=1)
    return lax.dynamic_update_slice_in_dim(joined, other, (1 - place) * width, axis=1)


def own_columns(array):
    width = array.shape[1] // lax.axis_size("tp")
    return lax.dynamic_slice_in_dim(array, lax.axis_index("tp") * width, width, axis=1)


def scattered(array):
    count = lax.axis_size("tp")
    if count > 2:
        return lax.psum_scatter(array, "tp", scatter_dimension=1, tiled=True).astype(f32)
    if count == 1:
        return array.astype(f32)
    width = array.shape[1] // 2
    place = lax.axis_index("tp")
    away = lax.dynamic_slice_in_dim(array, (1 - place) * width, width, axis=1)
    here = lax.ppermute(away, "tp", [(0, 1), (1, 0)])
    return own_columns(array).astype(f32) + here.astype(f32)


def swap_start(weight):
    count = lax.axis_size("inner")
    place = lax.axis_index("inner")
    width = weight.shape[1] // count
    pieces = []
    for turn in range(count):
        piece = lax.dynamic_slice_in_dim(weight, (place ^ turn) * width, width, axis=1)
        pieces.append(partner(piece, turn) if turn else piece)
    return pieces


def sum_tp(pair):
    if lax.axis_size("tp") == 2:
        return pair + lax.ppermute(pair, "tp", [(0, 1), (1, 0)])
    return lax.psum(pair, "tp")


def norm_scattered(added, residual, gain):
    total = resid_scale * residual.astype(f32) + added
    width = total.shape[1] * lax.axis_size("tp")
    sums = sum_tp(jnp.stack([jnp.sum(total, axis=1), jnp.sum(total * total, axis=1)]))
    mean = sums[0] / width
    variance = sums[1] / width - mean * mean
    return ((total - mean[:, None]) * lax.rsqrt(variance + norm_eps)[:, None] * gain).astype(bf16)


def spread(columns, heads_per):
    rows = columns.shape[0]
    lane = lax.broadcasted_iota(jnp.int32, (rows, 2 * HEAD_DIM), 1)
    pieces = []
    for pair in range(heads_per // 2):
        low = columns[:, 2 * pair : 2 * pair + 1]
        high = columns[:, 2 * pair + 1 : 2 * pair + 2]
        pieces.append(jnp.where(lane < HEAD_DIM, low, high))
    return jnp.concatenate(pieces, axis=1)


def mixer_kernel(
    value_ref, entry_ref, readout_ref,
    low_value_ref, low_entry_ref, low_readout_ref,
    high_value_ref, high_entry_ref, high_readout_ref,
    value_tap_ref, entry_tap_ref, readout_tap_ref,
    step_ref, sudden_ref, rate_ref, bias_ref, doc_ref, doc_row_ref, *rest,
    first_group,
):
    (out_ref, readout_out_ref, far_ref, end_ref,
     window, values, entries, fresh, starts, cols, lines) = rest[-11:]
    rows, width = value_ref.shape
    per = width // HEAD_DIM
    both = 2 * per
    blocks = rows // BLOCK
    taps = value_tap_ref.shape[0]
    half = taps // 2
    edge = 8
    pieces = [(value_ref, low_value_ref, high_value_ref, value_tap_ref, i * 128, i * 128)
              for i in range(width // 128)]
    pieces.append((entry_ref, low_entry_ref, high_entry_ref, entry_tap_ref, 0, width))
    pieces.append((readout_ref, low_readout_ref, high_readout_ref, readout_tap_ref, 0, width + 128))
    for source, low, high, _, at, to in pieces:
        window[0:edge, to : to + 128] = low[:, at : at + 128].astype(f32)
        window[edge + rows : 2 * edge + rows, to : to + 128] = high[:, at : at + 128].astype(f32)
        window[edge : edge + rows, to : to + 128] = source[:, at : at + 128].astype(f32)

    heads = step_ref.shape[1]
    wide = blocks * both
    first_head = (first_group + pl.program_id(0)) * per
    head = lax.broadcasted_iota(jnp.int32, (heads, wide), 0)
    lane = lax.broadcasted_iota(jnp.int32, (heads, wide), 1)
    at = lax.broadcasted_iota(jnp.int32, (BLOCK, BLOCK), 0)
    source_at = lax.broadcasted_iota(jnp.int32, (BLOCK, BLOCK), 1)
    lower = jnp.where(at >= source_at, 1.0, 0.0)
    unit = jnp.where(at == source_at, 1.0, 0.0)
    block_lane = lax.broadcasted_iota(jnp.int32, (1, wide), 1)
    ahead_lane = block_lane % both < per
    raw = jnp.zeros((BLOCK, wide), f32)
    sudden = jnp.zeros((BLOCK, wide), f32)
    own = jnp.zeros((BLOCK, wide), f32)
    before = jnp.zeros((1, wide), f32)
    after = jnp.zeros((1, wide), f32)
    for b in range(blocks):
        here = slice(b * BLOCK, (b + 1) * BLOCK)
        pick = (lane // both == b) & (head == first_head + lane % per)
        pick = jnp.where(pick, 1.0, 0.0)
        raw = raw + jnp.dot(step_ref[here, :], pick.astype(bf16), preferred_element_type=f32)
        sudden = sudden + jnp.dot(
            sudden_ref[here, :], pick, precision=exact_prec, preferred_element_type=f32
        )
        mine = block_lane // both == b
        top = edge + b * BLOCK
        own = jnp.where(mine, doc_ref[top : top + BLOCK, :], own)
        before = jnp.where(mine, doc_ref[top - 1 : top, :], before)
        after = jnp.where(mine, doc_ref[top + BLOCK : top + BLOCK + 1, :], after)

    def along_lanes(ref):
        every = jnp.where(head == first_head + lane % per, 1.0, 0.0)
        both_ways = jnp.dot(ref[...], every, precision=exact_prec, preferred_element_type=f32)
        return jnp.where(ahead_lane, both_ways[0:1], both_ways[1:2])

    raw = raw + along_lanes(bias_ref)
    step = jnp.maximum(raw, 0.0) + jnp.log1p(jnp.exp(-jnp.abs(raw)))
    decay = (sudden - jnp.exp(along_lanes(rate_ref)) * step) * LOG2E
    cum = jnp.dot(lower, decay, precision=exact_prec, preferred_element_type=f32)
    total = cum[BLOCK - 1 : BLOCK]
    cum = jnp.where(ahead_lane, cum, total - cum + decay)
    leave = jnp.where(ahead_lane, own[BLOCK - 1 : BLOCK], own[0:1])
    come = jnp.where(ahead_lane, before, after)
    outward = jnp.where(own == leave, jnp.exp2(total - cum) * step, 0.0)
    arrive = jnp.where(own == come, jnp.exp2(cum), 0.0)
    passing = jnp.where(leave == come, jnp.exp2(total), 0.0)
    row = lax.broadcasted_iota(jnp.int32, (wide, wide), 0)
    col = lax.broadcasted_iota(jnp.int32, (wide, wide), 1)
    forward_col = col % both < per
    nearer = (forward_col & (row < col)) | ((col % both >= per) & (row > col))
    between = jnp.where((row % both == col % both) & nearer, 1.0, 0.0)
    offset = jnp.dot(
        jnp.broadcast_to(total, (8, wide)), between, precision=exact_prec, preferred_element_type=f32
    )[0:1]
    turned = (row // both == col // both) & (row % per == col % per) & (row != col)
    other_step = jnp.dot(
        step, jnp.where(turned, 1.0, 0.0), precision=exact_prec, preferred_element_type=f32
    )
    prev_doc = doc_ref[edge - 1 : edge, :]
    next_doc = doc_ref[edge + rows : edge + rows + 1, :]
    beyond = jnp.where(ahead_lane, prev_doc, next_doc)
    far = jnp.where(own == beyond, jnp.exp2(cum + offset), 0.0)
    whole = jnp.where(beyond == leave, jnp.exp2(total + offset), 0.0)
    for k, part in enumerate((jnp.log2(step) - cum, jnp.log2(step + other_step))):
        lines[k * wide : (k + 1) * wide] = lax.dot_general(
            part, unit, (((0,), (0,)), ((), ())), precision=exact_prec, preferred_element_type=f32
        )
    for b in range(blocks):
        span = slice(b * both, (b + 1) * both)
        cols[b, :, 0:both] = cum[:, span]
        cols[b, :, both : 2 * both] = arrive[:, span]
        cols[b, :, 2 * both : 3 * both] = outward[:, span]
        far_ref[b * BLOCK : (b + 1) * BLOCK, :] = far[:, span]

    def conv_block(b, _):
        start = pl.multiple_of(b * BLOCK, BLOCK)
        here = pl.ds(start, BLOCK)
        docs = doc_ref[pl.ds(start, BLOCK + 2 * edge), :]
        own = docs[edge : edge + BLOCK]
        masks = [
            jnp.where(docs[edge - half + k : edge - half + k + BLOCK] == own, 1.0, 0.0)
            for k in range(taps)
        ]
        outward = cols[b, :, 2 * both : 3 * both]
        value_parts = []
        for source, low, high, tap_ref, at, to in pieces:
            around = window[pl.ds(start, BLOCK + 2 * edge), to : to + 128]
            acc = jnp.zeros((BLOCK, 128), f32)
            for k in range(taps):
                moved = around[edge - half + k : edge - half + k + BLOCK]
                term = moved * tap_ref[k : k + 1, at : at + 128].astype(f32)
                if k != half:
                    term = term * masks[k]
                acc = acc + term
            active = 0.5 * acc * (1.0 + jnp.tanh(0.5 * acc))
            if to < width:
                value_parts.append(active)
            elif to == width:
                entry = active.astype(bf16)
            else:
                readout_out_ref[here, :] = active.astype(bf16)
        value = jnp.concatenate(value_parts, axis=1)
        values[here, :] = value.astype(bf16)
        entries[here, :] = entry
        forward = value * spread(outward[:, :per], per)
        backward = value * spread(outward[:, per:], per)
        weighted = jnp.concatenate([forward, backward], axis=1).astype(bf16)
        fresh[b] = lax.dot_general(
            entry, weighted, (((0,), (0,)), ((), ())), preferred_element_type=f32
        )
        return 0

    lax.fori_loop(0, blocks, conv_block, 0, unroll=2)

    tail_row = lax.broadcasted_iota(jnp.int32, (16, width), 0)
    for k, order in ((0, range(blocks)), (1, range(blocks - 1, -1, -1))):
        span = slice(k * width, (k + 1) * width)
        state = jnp.zeros((STATE, width), f32)
        for b in order:
            starts[b, :, span] = state.astype(bf16)
            factor = spread(passing[:, b * both + k * per : b * both + (k + 1) * per], per)
            state = state * factor + fresh[b, :, span]
        share = STATE // SIDE
        for q in range(SIDE):
            end_ref[q, k, 0:share] = state[q * share : (q + 1) * share].astype(bf16)
        edge_block = (blocks - 1, 0)[k] * both + k * per
        factor = spread(whole[:, edge_block : edge_block + per], per)
        coarse = factor.astype(bf16).astype(f32)
        tail = jnp.where(tail_row == 0, coarse, jnp.where(tail_row == 1, factor - coarse, 0.0))
        for q in range(SIDE):
            end_ref[q, k, share : share + 16] = tail.astype(bf16)

    def out_block(b, _):
        start = pl.multiple_of(b * BLOCK, BLOCK)
        here = pl.ds(start, BLOCK)
        own = doc_ref[pl.ds(start + edge, BLOCK), :]
        cum = cols[b, :, 0:both]
        arrive = cols[b, :, both : 2 * both]
        along = lines[pl.ds(pl.multiple_of(b * both, both), both), :]
        singles = lines[pl.ds(pl.multiple_of(wide + b * both, both), both), :]
        readout = readout_out_ref[here, :]
        entry = entries[here, :]
        value = values[here, :]
        scores = lax.dot_general(
            readout, entry, (((1,), (1,)), ((), ())), preferred_element_type=f32
        )
        scores = jnp.where(own == doc_row_ref[b], scores, 0.0)
        at = lax.broadcasted_iota(jnp.int32, (BLOCK, BLOCK), 0)
        source_at = lax.broadcasted_iota(jnp.int32, (BLOCK, BLOCK), 1)
        value_lane = lax.broadcasted_iota(jnp.int32, (BLOCK, width), 1)
        weights = []
        spreads = []
        for r in range(per):
            ahead = cum[:, r : r + 1] + along[r : r + 1, :]
            behind = cum[:, per + r : per + r + 1] + along[per + r : per + r + 1, :]
            single = singles[r : r + 1, :]
            power = jnp.where(at > source_at, ahead, jnp.where(at < source_at, behind, single))
            weights.append((scores * jnp.exp2(power)).astype(bf16))
            mine = (value_lane >= r * HEAD_DIM) & (value_lane < (r + 1) * HEAD_DIM)
            spreads.append(jnp.where(mine, value, jnp.zeros_like(value)))
        total = jnp.dot(
            jnp.concatenate(weights, axis=1),
            jnp.concatenate(spreads, axis=0),
            preferred_element_type=f32,
        )
        carried = jnp.dot(readout, starts[b], preferred_element_type=f32)
        total = total + carried[:, 0:width] * spread(arrive[:, :per], per)
        total = total + carried[:, width : 2 * width] * spread(arrive[:, per:], per)
        out_ref[here, :] = total
        return 0

    lax.fori_loop(0, blocks, out_block, 0, unroll=2)


def opened(packed):
    rows = packed.shape[0] - 16
    factor = packed[rows : rows + 1, :].astype(f32) + packed[rows + 1 : rows + 2, :].astype(f32)
    return packed[0:rows, :].astype(f32), factor


def closed(pair):
    state, factor = pair
    tail_row = lax.broadcasted_iota(jnp.int32, (16, state.shape[1]), 0)
    coarse = factor.astype(bf16).astype(f32)
    tail = jnp.where(tail_row == 0, coarse, jnp.where(tail_row == 1, factor - coarse, 0.0))
    return jnp.concatenate([state, tail], axis=0).astype(bf16)


def chained(earlier, later):
    return earlier[0] * later[1] + later[0], earlier[1] * later[1]


def whole_kernel(place_ref, *refs):
    pieces, (ahead_ref, behind_ref, ordered) = refs[:-3], refs[-3:]
    for turn, piece in enumerate(pieces):
        ordered[place_ref[0] ^ turn] = piece[...]
    for k, order, out in ((0, (1, 2, 3), ahead_ref), (1, (2, 1, 0), behind_ref)):
        total = opened(ordered[0 if k == 0 else SIDE - 1, k])
        for j in order:
            total = chained(total, opened(ordered[j, k]))
        out[...] = closed(total)


def arrive_kernel(place_ref, *refs):
    pieces, others, (out_ref, ordered, arrived) = refs[:SIDE], refs[SIDE:-3], refs[-3:]
    for turn, piece in enumerate(pieces):
        ordered[place_ref[0] ^ turn] = piece[...]
    count = len(others) // 2
    width = pieces[0].shape[2]
    for k, order in ((0, range(SIDE)), (1, range(SIDE - 1, -1, -1))):
        total = opened(others[k * count])
        for other in others[k * count + 1 : (k + 1) * count]:
            total = chained(opened(other), total)
        for j in order:
            arrived[j, :, k * width : (k + 1) * width] = total[0].astype(bf16)
            total = chained(total, opened(ordered[j, k]))
    for turn in range(SIDE):
        out_ref[turn] = arrived[place_ref[0] ^ turn]


def gate_kernel(place_ref, *refs):
    mixed_ref, readout_ref, far_ref, gate_ref, gain_ref = refs[:5]
    pieces, out_ref, state_ref = refs[5:-2], refs[-2], refs[-1]
    rows, width = mixed_ref.shape
    per = width // HEAD_DIM
    share = STATE // SIDE
    for turn, piece in enumerate(pieces):
        at = pl.multiple_of((place_ref[0] ^ turn) * share, share)
        state_ref[pl.ds(at, share), :] = piece[...]

    def one(b, _):
        here = pl.ds(pl.multiple_of(b * BLOCK, BLOCK), BLOCK)
        far = far_ref[here, :]
        carried = jnp.dot(readout_ref[here, :], state_ref[...], preferred_element_type=f32)
        total = mixed_ref[here, :]
        total = total + carried[:, 0:width] * spread(far[:, :per], per)
        total = total + carried[:, width : 2 * width] * spread(far[:, per:], per)
        gate = gate_ref[here, :].astype(f32)
        total = total * (0.5 * gate * (1.0 + jnp.tanh(0.5 * gate)))
        scale = lax.rsqrt(jnp.mean(total * total, axis=1, keepdims=True) + norm_eps)
        out_ref[here, :] = (total * scale * gain_ref[...]).astype(bf16)
        return 0

    lax.fori_loop(0, rows // BLOCK, one, 0, unroll=3)


def up_kernel(place_ref, inner_ref, *refs):
    pieces, (weight_ref, out_ref, rows_ref) = refs[:-3], refs[-3:]
    depth = pieces[0].shape[1]
    outer, turns, wide, tile = weight_ref.shape

    @pl.when(pl.program_id(0) == 0)
    def _():
        top = 0
        for own_ref, other_ref in zip(pieces[::2], pieces[1::2]):
            rows = own_ref.shape[0]
            for half, source in ((place_ref[0], own_ref), (1 - place_ref[0], other_ref)):
                for block in range(depth // wide):
                    group, turn = block // turns, block % turns
                    at = (group * turns + (inner_ref[0] ^ turn)) * wide
                    to = half * depth + block * wide
                    rows_ref[top : top + rows, pl.ds(pl.multiple_of(to, 128), wide)] = source[
                        :, pl.ds(pl.multiple_of(at, 128), wide)
                    ]
            top += rows

    weight = weight_ref[...].reshape(outer * turns * wide, tile)
    hidden = jnp.dot(rows_ref[...], weight, preferred_element_type=f32)
    hidden = jnp.maximum(hidden, 0.0)
    out_ref[...] = (hidden * hidden).astype(bf16)


def up_rows(place, inner_place, pieces, weights):
    depth = pieces[0].shape[1]
    rows = sum(piece.shape[0] for piece in pieces[::2])
    outer, turns, wide, units = weights.shape
    tile = units // 4
    smem = pl.BlockSpec(memory_space=pltpu.SMEM)
    return pl.pallas_call(
        up_kernel,
        grid=(units // tile,),
        in_specs=[smem, smem] + [pl.BlockSpec(p.shape, lambda i: (0, 0)) for p in pieces] + [
            pl.BlockSpec((outer, turns, wide, tile), lambda i: (0, 0, 0, i)),
        ],
        out_specs=pl.BlockSpec((rows, tile), lambda i: (0, i)),
        out_shape=jax.ShapeDtypeStruct((rows, units), bf16),
        scratch_shapes=[pltpu.VMEM((rows, 2 * depth), bf16)],
        name="up_rows",
    )(place, inner_place, *pieces, weights)


def down_kernel(place_ref, inner_ref, *refs):
    pieces, (weight_ref, out_ref) = refs[:-2], refs[-2:]
    turns, wide, units = weight_ref.shape
    weight = weight_ref[...].reshape(turns * wide, units)
    at = 0
    for piece in pieces:
        rows = piece.shape[0]
        product = lax.dot_general(
            piece[...], weight, (((1,), (1,)), ((), ())), preferred_element_type=f32
        ).astype(bf16)
        for turn in range(turns):
            to = pl.multiple_of((inner_ref[0] ^ turn) * wide, 128)
            out_ref[at : at + rows, pl.ds(to, wide)] = product[:, turn * wide : (turn + 1) * wide]
        at += rows


def down_rows(place, inner_place, pieces, weights):
    rows = sum(piece.shape[0] for piece in pieces)
    outer, turns, wide, units = weights.shape
    half = outer // 2
    grid_spec = pltpu.PrefetchScalarGridSpec(
        num_scalar_prefetch=2,
        grid=(outer,),
        in_specs=[pl.BlockSpec(piece.shape, lambda i, place, inner: (0, 0)) for piece in pieces] + [
            pl.BlockSpec(
                (pl.Squeezed(), turns, wide, units),
                lambda i, place, inner: ((i + place[0] * half) % outer, 0, 0, 0),
            )
        ],
        out_specs=pl.BlockSpec(
            (pl.Squeezed(), rows, turns * wide), lambda i, place, inner: (i // half, 0, i % half)
        ),
    )
    return pl.pallas_call(
        down_kernel,
        grid_spec=grid_spec,
        out_shape=jax.ShapeDtypeStruct((2, rows, half * turns * wide), bf16),
        name="down_rows",
    )(place, inner_place, *pieces, weights)


def piece_kernel(here_ref, other_ref, *out_refs):
    at = 0
    for out_ref in out_refs:
        span = slice(at, at + out_ref.shape[0])
        out_ref[...] = (here_ref[span].astype(f32) + other_ref[span].astype(f32)).astype(bf16)
        at += out_ref.shape[0]


def summed_pieces(both, other, count):
    rows, width = other.shape
    shape = jax.ShapeDtypeStruct((rows // count, width), bf16)
    return pl.pallas_call(
        piece_kernel,
        grid=(1,),
        in_specs=[
            pl.BlockSpec((pl.Squeezed(), rows, width), lambda i: (0, 0, 0)),
            pl.BlockSpec((rows, width), lambda i: (0, 0)),
        ],
        out_specs=[pl.BlockSpec(shape.shape, lambda i: (0, 0))] * count,
        out_shape=[shape] * count,
        name="summed_pieces",
    )(both, other)


def in_order(weights):
    place = lax.axis_index("inner")
    turns = [lax.dynamic_index_in_dim(weights, place ^ j, 1, keepdims=True) for j in range(SIDE)]
    return jnp.concatenate(turns, axis=1).reshape(-1, weights.shape[3])


def norm_kernel(place_ref, *refs):
    parts, (stream_ref, gain_ref, own_ref, other_ref) = refs[:-4], refs[-4:]
    total = resid_scale * stream_ref[...].astype(f32)
    added = parts[0][...].astype(f32)
    for part in parts[1:]:
        added = added + part[...].astype(f32)
    total = total + added
    width = total.shape[1]
    mean = jnp.sum(total, axis=1, keepdims=True) / width
    variance = jnp.sum(total * total, axis=1, keepdims=True) / width - mean * mean
    normed = (total - mean) * lax.rsqrt(variance + norm_eps) * gain_ref[...]
    left, right = normed[:, : width // 2], normed[:, width // 2 :]
    first = place_ref[0] == 0
    own_ref[...] = jnp.where(first, left, right).astype(bf16)
    other_ref[...] = jnp.where(first, right, left).astype(bf16)


def norm_rows(place, parts, stream, gain):
    rows, width = stream.shape
    tile = min(rows, BLOCK)
    spec = pl.BlockSpec((tile, width), lambda i: (i, 0))
    half_spec = pl.BlockSpec((tile, width // 2), lambda i: (i, 0))
    return pl.pallas_call(
        norm_kernel,
        grid=(rows // tile,),
        in_specs=[pl.BlockSpec(memory_space=pltpu.SMEM)] + [spec] * (len(parts) + 1)
        + [pl.BlockSpec((1, width), lambda i: (0, 0))],
        out_specs=[half_spec] * 2,
        out_shape=[jax.ShapeDtypeStruct((rows, width // 2), bf16)] * 2,
        name="norm_rows",
    )(place, *parts, stream, gain)


def per_device(
    head_value_rows,
    entry_map_rows,
    readout_map_rows,
    output_gate_rows,
    step_before_softplus,
    sudden_log_decay,
    document_index,
    head_rate_logarithm,
    head_step_bias,
    value_conv_taps,
    entry_conv_taps,
    readout_conv_taps,
    group_norm_gain,
    mixer_output_weight,
    stream,
    mixer_norm_gain,
    channel_norm_gain,
    up_projection_weight,
    down_projection_weight,
):
    row_count = head_value_rows.shape[0]
    head_count = step_before_softplus.shape[1]
    groups = entry_map_rows.shape[1] // STATE
    per = head_count // groups
    width = per * HEAD_DIM
    blocks = row_count // BLOCK
    taps = value_conv_taps.shape[0]
    edge = 8

    joined_low = jnp.concatenate(
        [a[-edge:] for a in (head_value_rows, entry_map_rows, readout_map_rows)], axis=1
    )
    joined_high = jnp.concatenate(
        [a[:edge] for a in (head_value_rows, entry_map_rows, readout_map_rows)], axis=1
    )
    low = shifted(joined_low, 1)
    high = shifted(joined_high, -1)
    up_swaps = swap_start(up_projection_weight)
    (low, high), up_swaps, down_own = together((low, high), up_swaps, down_projection_weight)
    up_weights = lax.all_gather(jnp.stack(up_swaps), "outer")
    down_swaps = swap_start(down_own)

    position = lax.axis_index(SP) * row_count
    doc_pad = jnp.pad(document_index, edge, constant_values=-1)
    around = lax.dynamic_slice_in_dim(doc_pad, position, row_count + 2 * edge).astype(f32)
    doc_column = around[:, None]
    doc_rows = around[edge : edge + row_count].reshape(blocks, 1, BLOCK)

    def rows_spec(columns_wide, first=0):
        return pl.BlockSpec((row_count, columns_wide), lambda g: (0, first + g))

    def thin_spec(height, columns_wide, first=0):
        return pl.BlockSpec((height, columns_wide), lambda g: (0, first + g))

    def group_spec(*shape, first=0):
        return pl.BlockSpec(
            (pl.Squeezed(),) + shape, lambda g: (first + g,) + (0,) * len(shape)
        )

    def same_spec(*shape):
        return pl.BlockSpec(shape, lambda g: (0,) * len(shape))

    value_width, map_width = groups * width, groups * STATE
    share = STATE // SIDE
    pack_rows = share + 16

    def mixer(first, count, so_far):
        edge_specs = [
            thin_spec(edge, width, first),
            thin_spec(edge, STATE, value_width // STATE + first),
            thin_spec(edge, STATE, (value_width + map_width) // STATE + first),
        ]
        given = [
            head_value_rows, entry_map_rows, readout_map_rows, low, low, low, high, high, high,
            value_conv_taps, entry_conv_taps, readout_conv_taps, step_before_softplus,
            sudden_log_decay, head_rate_logarithm, head_step_bias, doc_column, doc_rows,
        ]
        return pl.pallas_call(
            functools.partial(mixer_kernel, first_group=first),
            grid=(count,),
            in_specs=[
                rows_spec(width, first), rows_spec(STATE, first), rows_spec(STATE, first),
                *edge_specs, *edge_specs,
                thin_spec(taps, width, first), thin_spec(taps, STATE, first),
                thin_spec(taps, STATE, first),
                same_spec(row_count, head_count), same_spec(row_count, head_count),
                same_spec(2, head_count), same_spec(2, head_count),
                same_spec(row_count + 2 * edge, 1), same_spec(blocks, 1, BLOCK),
            ] + [pl.BlockSpec(memory_space=pl.ANY)] * len(so_far),
            out_specs=[
                rows_spec(width, first), rows_spec(STATE, first),
                group_spec(row_count, 2 * per, first=first),
                pl.BlockSpec(
                    (SIDE, 2, pl.Squeezed(), pack_rows, width), lambda g: (0, 0, first + g, 0, 0)
                ),
            ],
            out_shape=[
                jax.ShapeDtypeStruct((row_count, groups * width), f32),
                jax.ShapeDtypeStruct((row_count, groups * STATE), bf16),
                jax.ShapeDtypeStruct((groups, row_count, 2 * per), f32),
                jax.ShapeDtypeStruct((SIDE, 2, groups, pack_rows, width), bf16),
            ],
            input_output_aliases={len(given) + i: i for i in range(len(so_far))},
            scratch_shapes=[
                pltpu.VMEM((row_count + 2 * edge, width + 2 * STATE), f32),
                pltpu.VMEM((row_count, width), bf16),
                pltpu.VMEM((row_count, STATE), bf16),
                pltpu.VMEM((blocks, STATE, 2 * width), f32),
                pltpu.VMEM((blocks, STATE, 2 * width), bf16),
                pltpu.VMEM((blocks, BLOCK, 128), f32),
                pltpu.VMEM((4 * per * blocks, BLOCK), f32),
            ],
            name="mixer",
        )(*given, *so_far)

    local, readouts, far, ends = mixer(0, groups, [])

    reach = min(lax.axis_size(SP) - 1, -(-(MAX_DOCUMENT - 1) // row_count))
    spans = -(-reach // SIDE)
    inner_place = lax.axis_index("inner").astype(jnp.int32)[None]

    def share_of(array, turn):
        return lax.dynamic_index_in_dim(array, lax.axis_index("inner") ^ turn, 0, keepdims=False)

    shares = [share_of(ends, 0)] + [partner(share_of(ends, turn), turn) for turn in (1, 2, 3)]
    smem = pl.BlockSpec(memory_space=pltpu.SMEM)
    share_spec = pl.BlockSpec((2, pl.Squeezed(), pack_rows, width), lambda g: (0, g, 0, 0))
    pack_spec = group_spec(pack_rows, width)
    pack_shape = jax.ShapeDtypeStruct((groups, pack_rows, width), bf16)
    ordered = pltpu.VMEM((SIDE, 2, pack_rows, width), bf16)
    ahead, behind = pl.pallas_call(
        whole_kernel,
        grid=(groups,),
        in_specs=[smem] + [share_spec] * SIDE,
        out_specs=[pack_spec] * 2,
        out_shape=[pack_shape] * 2,
        scratch_shapes=[ordered],
        name="whole",
    )(inner_place, *shares)
    others = [shifted(ahead, j, "outer") for j in range(1, spans + 1)]
    others = others + [shifted(behind, -j, "outer") for j in range(1, spans + 1)]
    arrivals = pl.pallas_call(
        arrive_kernel,
        grid=(groups,),
        in_specs=[smem] + [share_spec] * SIDE + [pack_spec] * len(others),
        out_specs=pl.BlockSpec((SIDE, pl.Squeezed(), share, 2 * width), lambda g: (0, g, 0, 0)),
        out_shape=jax.ShapeDtypeStruct((SIDE, groups, share, 2 * width), bf16),
        scratch_shapes=[ordered, pltpu.VMEM((SIDE, share, 2 * width), bf16)],
        name="arrive",
    )(inner_place, *shares, *others)
    packs = [arrivals[0]] + [partner(arrivals[turn], turn) for turn in (1, 2, 3)]
    down_weights = lax.all_gather(jnp.stack(down_swaps), "outer")

    tp_count = lax.axis_size("tp")
    if tp_count == 2:
        stream_full = columns_over_tp(stream)
        gain_one = columns_over_tp(mixer_norm_gain[None])
        packs, stream_full, gain_one = together(packs, stream_full, gain_one)
    normed = pl.pallas_call(
        gate_kernel,
        grid=(groups,),
        in_specs=[
            smem, rows_spec(width), rows_spec(STATE), group_spec(row_count, 2 * per),
            rows_spec(width), thin_spec(1, width),
        ] + [group_spec(share, 2 * width)] * SIDE,
        out_specs=rows_spec(width),
        out_shape=jax.ShapeDtypeStruct((row_count, groups * width), bf16),
        scratch_shapes=[pltpu.VMEM((STATE, 2 * width), bf16)],
        name="gate",
    )(inner_place, local, readouts, far, output_gate_rows, group_norm_gain[None], *packs)

    part = jnp.dot(normed, mixer_output_weight, preferred_element_type=f32).astype(bf16)
    place = lax.axis_index("tp").astype(jnp.int32)[None]
    if tp_count == 2:
        own_one, other_one = norm_rows(place, over_tp(part), stream_full, gain_one)
    else:
        own_one = norm_scattered(scattered(part), stream, mixer_norm_gain)
        other_one = None

    def hidden_units(pieces, others=None):
        if tp_count == 2:
            others = [over_tp(rows)[1] for rows in pieces] if others is None else others
            pairs = [array for pair in zip(pieces, others) for array in pair]
            return up_rows(place, inner_place, pairs, up_weights)
        up = in_order(up_weights)
        rows = columns_over_tp(jnp.concatenate(pieces, axis=0))
        hidden = jnp.dot(rows, up, preferred_element_type=f32)
        return jnp.square(jax.nn.relu(hidden)).astype(bf16)

    def contributions(pieces, count=1):
        if tp_count == 2:
            both = down_rows(place, inner_place, pieces, down_weights)
            other = lax.ppermute(both[1], "tp", [(0, 1), (1, 0)])
            if count > 1:
                return summed_pieces(both, other, count)
            return (both[0].astype(f32) + other.astype(f32)).astype(bf16)
        down = in_order(down_weights)
        product = lax.dot_general(
            jnp.concatenate(pieces, axis=0), down, (((1,), (1,)), ((), ())),
            preferred_element_type=f32,
        )
        total = scattered(product.astype(bf16)).astype(bf16)
        return jnp.split(total, count, axis=0) if count > 1 else total

    middle = row_count // 2
    side_one, side_two = partner(own_one, 1), partner(own_one, 2)
    units = hidden_units([own_one], [other_one])
    side_one, side_two, units = together(side_one, side_two, units)
    far_one = partner(side_one[:middle], 2)
    far_two = partner(side_two[middle:], 1)
    near_units = hidden_units([side_one, side_two])
    near_units, far_one, far_two = together(near_units, far_one, far_two)
    late_one, ready_one, ready_two, late_two = contributions([near_units], 4)
    early_one = partner(ready_one, 1)
    early_two = partner(ready_two, 2)
    diagonal_units = hidden_units([far_one, far_two])
    for_hop_one, for_hop_two = contributions([diagonal_units], 2)
    hop_one = partner(for_hop_one, 2)
    hop_two = partner(for_hop_two, 1)
    own_sum = contributions([units])
    late_one = partner(late_one + hop_one, 1)
    late_two = partner(late_two + hop_two, 2)
    back_one = jnp.concatenate([late_one, early_one], axis=0).astype(f32)
    back_two = jnp.concatenate([early_two, late_two], axis=0).astype(f32)
    added = own_sum.astype(f32) + back_one + back_two
    return norm_scattered(added, own_one, channel_norm_gain)


def solution(mesh):
    sp_count, tp_count = mesh.devices.shape
    inner = SIDE
    finer = jax.sharding.Mesh(
        mesh.devices.reshape(sp_count // inner, inner, tp_count), ("outer", "inner", "tp")
    )
    both = P(SP, "tp")
    second = P(None, "tp")
    placed = (
        both, both, both, both, both, both, P(), second, second, second, second, second,
        P("tp"), P("tp", None), both, P("tp"), P("tp"), both, both,
    )
    return jax.shard_map(
        per_device, mesh=finer, in_specs=placed, out_specs=both, check_vma=False
    )
```
